256 devices in a mesh: sp: 64 (over z, x, core), tp: 4 (over y).
Axes of the slice: x: 4, y: 4, z: 8, core: 2. Of those that a mesh axis runs over, the one named last changes fastest.
Arguments:
- tokens: bfloat16 [12288, 2048], P(('sp', 'tp')), may hold values from -54 to 54
- w_query: bfloat16 [2048, 2048], P(None, 'tp'), may hold values from -0.21875 to 0.21875
- w_key: bfloat16 [2048, 2048], P(None, 'tp'), may hold values from -0.125 to 0.125
- w_value: bfloat16 [2048, 2048], P(None, 'tp'), may hold values from -0.125 to 0.125
- w_out: bfloat16 [2048, 2048], P('tp'), may hold values from -0.125 to 0.125
- mix_weight: float32 [16], P('tp'), may hold values from 0.3 to 0.8
- out_gain: float32 [128], replicated, may hold values from 0.1 to 1.9
Outputs:
- mixed: bfloat16 [12288, 2048], P(('sp', 'tp'))
The draws below stay inside these ranges and needn't reach their ends.
All inputs are finite; a program needn't handle non-finite values.
Results may differ from the reference program's by a relative error of at most 0.018.
The reference program's roundings to bfloat16 on the way (of `queries`, `keys`, `values`, `weights` and `normed`) count: a program that leaves them out, or rounds other values in their place, can miss the bound.
Values may be sent and summed in bfloat16 or wider, within the bound.
A program may use at most 192 MiB of HBM per device.

```python
import math
import jax
import jax.numpy as jnp
from jax import lax

D = 2048
HEADS = 16
HD = 64
VD = 128
TOKENS = 12288


def draw_tokens(key, part):
    key_noise = jax.random.fold_in(key, 11)
    key_dir = jax.random.fold_in(key, 12)
    noise = jax.random.truncated_normal(key_noise, -6.0, 6.0, (TOKENS, D), jnp.float32)
    direction = jax.random.truncated_normal(key_dir, -6.0, 6.0, (D,), jnp.float32)
    place = jnp.arange(TOKENS, dtype=jnp.float32) / TOKENS
    drift = jnp.cos(3.14159265 * place)
    result = noise + drift[:, None] * direction[None, :]
    return result.astype(jnp.bfloat16)


def level_of(rng, shape, pieces, least, high):
    def one(position, shards_of):
        draws = jax.random.uniform(jax.random.fold_in(jax.random.fold_in(rng, 6), position), (shards_of,), jnp.float32, least / len(pieces), high / len(pieces))
        return jnp.repeat(jnp.exp(draws), shape[position] // shards_of).reshape((-1,) + (1,) * (len(shape) - position - 1))

    loudness = one(*pieces[0])
    for cut in pieces[1:]:
        loudness = loudness * one(*cut)
    return loudness


def gaussian(own_key, dims, deviation, reach, shards=(), held_as=jnp.bfloat16):
    values = jax.random.normal(own_key, dims, jnp.float32) * deviation
    if len(shards) > 0:
        values = level_of(own_key, dims, shards, -0.22, 0.18) * values
    return jnp.clip(values, min=-reach, max=reach).astype(held_as)


def setup_inputs(seed: int = 0) -> dict:
    seeds = jax.random.split(jax.random.key(seed), 8)
    tokens = draw_tokens(jax.random.fold_in(seeds[7], 71), 0)
    w_query = gaussian(seeds[1], (D, HEADS * 2 * HD), (D // 3) ** -0.5, 0.21875, ((1, 4),))
    w_key = gaussian(seeds[2], (D, HEADS * 2 * HD), D ** -0.5, 0.125, ((1, 4),))
    w_value = gaussian(seeds[3], (D, HEADS * VD), D ** -0.5, 0.125, ((1, 4),))
    w_out = gaussian(seeds[4], (HEADS * VD, D), (HEADS * VD) ** -0.5, 0.125, ((0, 4),))
    mix_weight = jnp.clip(0.3 + 0.5 * jax.random.uniform(seeds[5], (HEADS,), jnp.float32) ** level_of(seeds[5], (HEADS,), ((0, 4),), -0.2, 0.2), 0.3, 0.8)
    out_gain = jnp.clip(1.0 + 0.18 * jax.random.normal(seeds[6], (VD,), jnp.float32), 0.1, 1.9)
    return dict(tokens=tokens, w_query=w_query, w_key=w_key, w_value=w_value, w_out=w_out, mix_weight=mix_weight, out_gain=out_gain)


def one_head(args):
    query_h, key_h, value_h, lam = args
    block = math.gcd(TOKENS, 1024)
    query_blocks = query_h.reshape(TOKENS // block, block, 2, HD)
    key_f = key_h.astype(jnp.float32)
    value_f = value_h.astype(jnp.float32)

    def per_block(query_b):
        scores = jnp.einsum('qmd,kmd->mqk', query_b.astype(jnp.float32), key_f) * HD ** (-0.5)
        top = lax.optimization_barrier(jnp.max(scores, axis=-1, keepdims=True))
        expw = jnp.exp(scores - top)
        total = lax.optimization_barrier(jnp.sum(expw, axis=-1))
        weights = expw.astype(jnp.bfloat16).astype(jnp.float32)
        accum = jnp.einsum('mqk,ke->mqe', weights, value_f)
        return accum[0] / total[0][:, None] - lam * accum[1] / total[1][:, None]
    return lax.map(per_block, query_blocks).reshape(TOKENS, VD)

def reference(tokens, w_query, w_key, w_value, w_out, mix_weight, out_gain):
    queries = jnp.dot(tokens, w_query, preferred_element_type=jnp.float32).astype(jnp.bfloat16)
    keys = jnp.dot(tokens, w_key, preferred_element_type=jnp.float32).astype(jnp.bfloat16)
    values = jnp.dot(tokens, w_value, preferred_element_type=jnp.float32).astype(jnp.bfloat16)
    query_h = queries.reshape(TOKENS, HEADS, 2, HD).transpose(1, 0, 2, 3)
    key_h = keys.reshape(TOKENS, HEADS, 2, HD).transpose(1, 0, 2, 3)
    value_h = values.reshape(TOKENS, HEADS, VD).transpose(1, 0, 2)
    heads_out = lax.map(one_head, (query_h, key_h, value_h, mix_weight))
    meansq = lax.optimization_barrier(jnp.mean(heads_out * heads_out, axis=-1, keepdims=True))
    normed = (heads_out * lax.rsqrt(meansq + 1e-06) * out_gain).astype(jnp.bfloat16)
    normed = normed.transpose(1, 0, 2).reshape(TOKENS, HEADS * VD)
    return jnp.dot(normed, w_out, preferred_element_type=jnp.float32).astype(jnp.bfloat16)
```

```python
import functools

import jax
import jax.numpy as jnp
from jax import lax
from jax.experimental import pallas as pl
from jax.experimental.pallas import tpu as pltpu
from jax.sharding import PartitionSpec as P

MESH = pl.DeviceIdType.MESH
NX = 4
NY = 4
NC = 2
Y_OFFSET = (0, 1, 3, 2)
BF16 = jnp.bfloat16
F32 = jnp.float32


def kernel(
    nz,
    rows,
    tok_hbm,
    wq_hbm,
    wk_hbm,
    wv_hbm,
    wo_hbm,
    lam_ref,
    gain_ref,
    out_ref,
    tok,
    wkvq,
    wo,
    send_kv,
    send_q,
    qbuf,
    kv,
    qw,
    top,
    total,
    acc,
    nbuf,
    mixin,
    load_sem,
    y_send,
    y_recv,
    x_send,
    x_recv,
    q_send,
    q_recv,
    r_send,
    r_recv,
    s_send,
    s_recv,
    wo_send,
    wo_recv,
    ws_send,
    ws_recv,
    o_send,
    o_recv,
):
    half = nz // 2
    whole_events = (half - 1) * 4
    events = whole_events + 2
    depth = tok.shape[-1]
    group = NX * rows
    queries = NY * group
    tiles = queries // 128
    out_rows = wo_hbm.shape[0]
    out_cols = wo.shape[-1]

    sp = lax.axis_index("sp")
    y = lax.axis_index("tp")
    c = lax.rem(sp, NC)
    x = lax.rem(sp // NC, NX)
    z = sp // (NC * NX)

    def device(zz, xx, cc, yy):
        return {"sp": (zz * NX + xx) * NC + cc, "tp": yy}

    def around(value, step, count):
        return lax.rem(value + (step % count), count)

    def remote(src, dst, send, recv, where):
        return pltpu.make_async_remote_copy(
            src_ref=src,
            dst_ref=dst,
            send_sem=send,
            recv_sem=recv,
            device_id=where,
            device_id_type=MESH,
        )

    up = device(z, x, c, around(y, 1, NY))
    down = device(z, x, c, around(y, -1, NY))
    right = device(around(z, 1, nz), x, c, y)
    left = device(around(z, -1, nz), x, c, y)
    sibling = device(z, x, 1 - c, y)

    loads = []
    for part in range(2):
        loads.append(
            pltpu.make_async_copy(
                tok_hbm.at[:, pl.ds(part * depth, depth)], tok.at[0, part], load_sem.at[part]
            )
        )
    weight_loads = [
        pltpu.make_async_copy(w, wkvq.at[i], load_sem.at[2 + i])
        for i, w in enumerate((wk_hbm, wv_hbm, wq_hbm))
    ]
    wo_loads = [
        pltpu.make_async_copy(
            wo_hbm.at[:, pl.ds(part * out_cols, out_cols)], wo.at[y, part], load_sem.at[5 + part]
        )
        for part in range(2)
    ]
    for copy in loads + weight_loads + wo_loads:
        copy.start()

    barrier = pltpu.get_barrier_semaphore()
    peers = [right, left, sibling]
    for oy in range(NY):
        for ox in range(NX):
            if (oy, ox) != (0, 0):
                peers.append(device(z, around(x, ox, NX), c, around(y, oy, NY)))
    for peer in peers:
        pl.semaphore_signal(barrier, inc=1, device_id=peer, device_id_type=MESH)
    for copy in loads:
        copy.wait()
    pl.semaphore_wait(barrier, len(peers))

    def y_copy(slot, part):
        return remote(
            tok.at[0, part],
            tok.at[slot, part],
            y_send.at[slot, part],
            y_recv.at[slot, part],
            down if slot == 1 else up,
        )

    def y_relay(part):
        return remote(
            tok.at[2 if part == 0 else 1, part],
            tok.at[3, part],
            y_send.at[3, part],
            y_recv.at[3, part],
            up if part == 0 else down,
        )

    y_copy(2, 0).start()
    y_copy(1, 1).start()
    y_copy(2, 1).start()
    y_copy(1, 0).start()

    def x_copies(s, o):
        other = around(x, o, NX)
        source = around(x, -o, NX)
        to = device(z, other, c, y)
        mine = pl.ds(pl.multiple_of(s * group + x * rows, 16), rows)
        theirs = pl.ds(pl.multiple_of(s * group + source * rows, 16), rows)
        return (
            remote(send_kv.at[s, other], kv.at[0, mine], x_send.at[s, o], x_recv.at[s, o], to),
            remote(send_q.at[s, other], qbuf.at[mine], q_send.at[s, o], q_recv.at[s, o], to),
            remote(send_kv.at[s, other], kv.at[0, theirs], x_send.at[s, o], x_recv.at[s, o], to),
            remote(send_q.at[s, other], qbuf.at[theirs], q_send.at[s, o], q_recv.at[s, o], to),
        )

    def project(s):
        first = tok[s, 0]
        second = tok[s, 1]

        def product(i):
            out = jnp.dot(first, wkvq[i, :depth, :], preferred_element_type=F32)
            out += jnp.dot(second, wkvq[i, depth:, :], preferred_element_type=F32)
            return out.astype(BF16)

        mine = pl.ds(pl.multiple_of(s * group + x * rows, 16), rows)
        keys = product(0)
        values = product(1)
        for head in range(NX):
            cols = slice(head * 128, head * 128 + 128)
            send_kv[s, head, :, :128] = keys[:, cols]
            send_kv[s, head, :, 128:] = values[:, cols]
        for o in (2, 1, 3):
            x_copies(s, o)[0].start()
        kv[0, mine, :] = send_kv[s, x]
        found = product(2)
        for head in range(NX):
            send_q[s, head] = found[:, head * 128 : head * 128 + 128]
        for o in (2, 1, 3):
            x_copies(s, o)[1].start()
        qbuf[mine, :] = send_q[s, x]

    def ring_first(s, way):
        if half > 1:
            event = s
        elif (way == 0) == (s < 2):
            event = s % 2
        else:
            return None
        return remote(
            kv.at[0, pl.ds(s * group, group)],
            kv.at[2 + event, pl.ds(way * group, group)],
            r_send.at[s, way],
            r_recv.at[event, way],
            right if way == 0 else left,
        )

    def sibling_first(s):
        span = pl.ds(s * group, group)
        return remote(kv.at[0, span], kv.at[1, span], s_send.at[events + s], s_recv.at[events + s], sibling)

    def launch(s):
        for o in (1, 3, 2):
            x_copies(s, o)[2].wait_recv()
        for way in range(2):
            copy = ring_first(s, way)
            if copy is not None:
                copy.start()
        sibling_first(s).start()

    for copy in weight_loads:
        copy.wait()
    project(0)
    launch(0)
    y_copy(2, 0).wait_recv()
    y_relay(0).start()
    y_copy(1, 1).wait_recv()
    y_relay(1).start()
    y_copy(1, 0).wait_recv()
    project(1)
    y_copy(2, 1).wait_recv()
    project(2)
    launch(1)
    launch(2)

    def wo_span(part):
        size = out_rows // 2
        return pl.ds(part * size, size)

    def wo_copy(way, part):
        span = wo_span(part)
        return remote(
            wo.at[y, c, span],
            wo.at[y, c, span],
            wo_send.at[way, part],
            wo_recv.at[way, part],
            up if way == 0 else down,
        )

    def wo_arrival(way, part):
        origin = around(y, -1 if way == 0 else 1, NY)
        span = wo_span(part)
        return remote(
            wo.at[y, c, span],
            wo.at[origin, c, span],
            wo_send.at[way, part],
            wo_recv.at[way, part],
            up if way == 0 else down,
        )

    def wo_relay(part):
        origin = around(y, -1 if part == 0 else 1, NY)
        span = wo_span(part)
        return remote(
            wo.at[origin, c, span],
            wo.at[origin, c, span],
            wo_send.at[2, part],
            wo_recv.at[2, part],
            up if part == 0 else down,
        )

    def wo_relay_arrival(part):
        origin = around(y, 2, NY)
        span = wo_span(part)
        return remote(
            wo.at[y, c, span],
            wo.at[origin, c, span],
            wo_send.at[2, part],
            wo_recv.at[2, part],
            up if part == 0 else down,
        )

    def wo_sibling(way, part, core):
        origin = around(y, (-1, 1, 2)[way], NY)
        span = wo_span(part)
        return remote(
            wo.at[origin, core, span],
            wo.at[origin, core, span],
            ws_send.at[way, part],
            ws_recv.at[way, part],
            sibling,
        )

    for copy in wo_loads:
        copy.wait()

    y_relay_in = [
        remote(tok.at[0, part], tok.at[3, part], y_send.at[3, part], y_recv.at[3, part], up)
        for part in range(2)
    ]
    for copy in y_relay_in:
        copy.wait_recv()
    wo_copy(0, 0).start()
    wo_copy(1, 1).start()
    wo_copy(0, 1).start()
    wo_copy(1, 0).start()
    project(3)
    launch(3)

    for s in range(NY):
        for o in (1, 3, 2):
            x_copies(s, o)[3].wait_recv()
    upper = lax.broadcasted_iota(jnp.int32, (128, 128), 0) < 64

    def build(t, carry):
        block = qbuf[pl.ds(pl.multiple_of(t * 128, 128), 128), :].astype(F32) * (64**-0.5)
        block = block.T
        nothing = jnp.zeros_like(block)
        qw[t, :, :128] = jnp.where(upper, block, nothing).astype(BF16)
        qw[t, :, 128:] = jnp.where(upper, nothing, block).astype(BF16)
        return carry

    lax.fori_loop(0, tiles, build, 0)
    top[...] = jnp.full_like(top, -1e30)
    total[...] = jnp.zeros_like(total)
    acc[...] = jnp.zeros_like(acc)

    def arrival(e, way):
        return remote(
            kv.at[0, pl.ds(0, group)],
            kv.at[2 + e, pl.ds(way * group, group)],
            r_send.at[e, way],
            r_recv.at[e, way],
            right,
        )

    def forward(e, way, target):
        return remote(
            kv.at[2 + e, pl.ds(way * group, group)],
            kv.at[2 + target, pl.ds(way * group, group)],
            r_send.at[4 + e, way],
            r_recv.at[target, way],
            right if way == 0 else left,
        )

    def to_sibling(e):
        return remote(
            kv.at[2 + e, pl.ds(0, 2 * group)],
            kv.at[2 + e, pl.ds(2 * group, 2 * group)],
            s_send.at[e],
            s_recv.at[e],
            sibling,
        )

    def goes_left(e):
        target = jnp.where(e + 4 < whole_events, e + 4, e + 2)
        return (e + 4 < whole_events) | ((e < whole_events) & (lax.rem(e, 4) >= 2)), target

    def receive(e):
        arrival(e, 0).wait_recv()

        @pl.when(e + 4 < events)
        def _():
            forward(e, 0, e + 4).start()

        arrival(e, 1).wait_recv()
        moves, target = goes_left(e)

        @pl.when(moves)
        def _():
            forward(e, 1, target).start()

        to_sibling(e).start()

    def attend(u, carry):
        @pl.when(u == 1)
        def _():
            for s in range(NY):
                sibling_first(s).wait_recv()

        @pl.when(u >= 2)
        def _():
            to_sibling(u - 2).wait_recv()

        keys = kv[u, :, :128]
        values = kv[u, :, 128:].T
        for t in range(tiles):
            scores = jnp.dot(keys, qw[t], preferred_element_type=F32)
            before = top[t]
            now = jnp.maximum(before, jnp.max(scores, axis=0, keepdims=True))
            factor = jnp.exp(before - now)
            expw = jnp.exp(scores - now)
            top[t] = now
            total[t] = total[t] * factor + jnp.sum(expw, axis=0, keepdims=True)
            acc[t] = acc[t] * factor + jnp.dot(values, expw.astype(BF16), preferred_element_type=F32)
        return carry

    relay_at = events // 2

    def step(e, carry):
        receive(e)

        @pl.when(e == relay_at)
        def _():
            for part in range(2):
                wo_arrival(part, part).wait_recv()
                wo_relay(part).start()
                wo_sibling(part, part, c).start()

        begin = e + jnp.where(e >= 5, 1, 0)
        end = e + 1 + jnp.where(e >= 4, 1, 0)
        lax.fori_loop(begin, end, attend, 0)
        return carry

    lax.fori_loop(0, events, step, 0)
    for way in range(2):
        wo_arrival(way, 1 - way).wait_recv()
        wo_sibling(way, 1 - way, c).start()
    behind = events + (1 if events > 4 else 0)
    lax.fori_loop(behind, events + 2, attend, 0)

    mix = lam_ref[x]
    gain = gain_ref[...]

    def finish(t, carry):
        ratio = acc[t] / total[t]
        heads_out = ratio[:, :128] - mix * ratio[:, 128:]
        meansq = jnp.mean(heads_out * heads_out, axis=0, keepdims=True)
        normed = (heads_out * lax.rsqrt(meansq + 1e-06)).T * gain
        nbuf[pl.ds(pl.multiple_of(t * 128, 128), 128), :] = normed.astype(BF16)
        return carry

    lax.fori_loop(0, tiles, finish, 0, unroll=True)

    def o_copy(s, o, arriving):
        other = around(x, o, NX)
        span = pl.ds(pl.multiple_of(s * group + other * rows, 16), rows)
        if arriving:
            slot = around(y, -Y_OFFSET[s], NY) * NX + around(x, -o, NX)
        else:
            slot = y * NX + x
        return remote(
            nbuf.at[span],
            mixin.at[slot],
            o_send.at[s, o],
            o_recv.at[s, o],
            device(z, other, c, around(y, Y_OFFSET[s], NY)),
        )

    exchanges = [(s, o) for s in (3, 1, 2, 0) for o in (2, 1, 3, 0) if (s, o) != (0, 0)]
    for s, o in exchanges:
        o_copy(s, o, False).start()
    mixin[y * NX + x] = nbuf[pl.ds(pl.multiple_of(x * rows, 16), rows), :]

    for part in range(2):
        wo_relay_arrival(part).wait_recv()
        wo_sibling(2, part, c).start()
    for way in range(3):
        for part in range(2):
            wo_sibling(way, part, 1 - c).wait_recv()
    for s, o in exchanges:
        o_copy(s, o, True).wait_recv()
    normed = jnp.concatenate([mixin[h] for h in range(NX * NY)], axis=1)
    for part in range(2):
        mixed = jnp.zeros((rows, out_cols), F32)
        for yy in range(NY):
            span = slice(yy * out_rows, (yy + 1) * out_rows)
            mixed += jnp.dot(normed[:, span], wo[yy, part], preferred_element_type=F32)
        out_ref[:, part * out_cols : (part + 1) * out_cols] = mixed.astype(BF16)

    for part in range(2):
        for slot in (1, 2):
            y_copy(slot, part).wait_send()
        y_relay(part).wait_send()
    for s in range(NY):
        for o in (1, 2, 3):
            copies = x_copies(s, o)
            copies[0].wait_send()
            copies[1].wait_send()
        for way in range(2):
            copy = ring_first(s, way)
            if copy is not None:
                copy.wait_send()
        sibling_first(s).wait_send()

    def drain(e, carry):
        @pl.when(e + 4 < events)
        def _():
            forward(e, 0, e + 4).wait_send()

        moves, target = goes_left(e)

        @pl.when(moves)
        def _():
            forward(e, 1, target).wait_send()

        to_sibling(e).wait_send()
        return carry

    lax.fori_loop(0, events, drain, 0)
    for part in range(2):
        for way in range(2):
            wo_copy(way, part).wait_send()
        wo_relay(part).wait_send()
        for way in range(3):
            wo_sibling(way, part, c).wait_send()
    for s, o in exchanges:
        o_copy(s, o, False).wait_send()


def solution(mesh):
    nz = mesh.shape["sp"] // (NX * NC)

    def shards(tokens, w_query, w_key, w_value, w_out, mix_weight, out_gain):
        rows, width = tokens.shape
        cols = w_query.shape[1]
        group = NX * rows
        queries = NY * group
        tiles = queries // 128
        events = (nz // 2 - 1) * 4 + 2
        dma = pltpu.SemaphoreType.DMA
        anywhere = pl.BlockSpec(memory_space=pl.ANY)
        return pl.pallas_call(
            functools.partial(kernel, nz, rows),
            out_shape=jax.ShapeDtypeStruct((rows, width), BF16),
            in_specs=[anywhere] * 5
            + [pl.BlockSpec(memory_space=pltpu.SMEM), pl.BlockSpec(memory_space=pltpu.VMEM)],
            out_specs=pl.BlockSpec(memory_space=pltpu.VMEM),
            scratch_shapes=[
                pltpu.VMEM((NY, 2, rows, width // 2), BF16),
                pltpu.VMEM((3, width, cols), BF16),
                pltpu.VMEM((NY, 2, w_out.shape[0], width // 2), BF16),
                pltpu.VMEM((NY, NX, rows, 256), BF16),
                pltpu.VMEM((NY, NX, rows, 128), BF16),
                pltpu.VMEM((queries, 128), BF16),
                pltpu.VMEM((events + 2, 4 * group, 256), BF16),
                pltpu.VMEM((tiles, 128, 256), BF16),
                pltpu.VMEM((tiles, 1, 256), F32),
                pltpu.VMEM((tiles, 1, 256), F32),
                pltpu.VMEM((tiles, 128, 256), F32),
                pltpu.VMEM((queries, 128), BF16),
                pltpu.VMEM((NX * NY, rows, 128), BF16),
                dma((7,)),
                dma((4, 2)),
                dma((4, 2)),
                dma((4, 4)),
                dma((4, 4)),
                dma((4, 4)),
                dma((4, 4)),
                dma((events + 4, 2)),
                dma((events, 2)),
                dma((events + 4,)),
                dma((events + 4,)),
                dma((3, 2)),
                dma((3, 2)),
                dma((3, 2)),
                dma((3, 2)),
                dma((4, 4)),
                dma((4, 4)),
            ],
            compiler_params=pltpu.CompilerParams(
                collective_id=0,
                has_side_effects=True,
                vmem_limit_bytes=56 * 1024 * 1024,
            ),
        )(tokens, w_query, w_key, w_value, w_out, mix_weight, out_gain.reshape(1, -1))

    in_specs = (
        P(("sp", "tp"), None),
        P(None, "tp"),
        P(None, "tp"),
        P(None, "tp"),
        P("tp", None),
        P("tp"),
        P(),
    )
    return jax.shard_map(
        shards, mesh=mesh, in_specs=in_specs, out_specs=P(("sp", "tp"), None), check_vma=False
    )
```

```python
import functools

import jax
import jax.numpy as jnp
from jax import lax
from jax.experimental import pallas as pl
from jax.experimental.pallas import tpu as pltpu
from jax.sharding import PartitionSpec as P

MESH = pl.DeviceIdType.MESH
NX = 4
NY = 4
NC = 2
Y_OFFSET = (0, 1, 3, 2)
BF16 = jnp.bfloat16
F32 = jnp.float32
LOG2E = 1.4426950408889634


def kernel(
    nz,
    rows,
    tok_hbm,
    wq_hbm,
    wk_hbm,
    wv_hbm,
    wo_hbm,
    lam_ref,
    gain_ref,
    out_ref,
    tok,
    wkvq,
    wo,
    send_kv,
    send_q,
    qbuf,
    kv,
    qw,
    top,
    acc,
    nbuf,
    mixin,
    load_sem,
    y_send,
    y_recv,
    x_send,
    x_recv,
    q_send,
    q_recv,
    r_send,
    r_recv,
    s_send,
    s_recv,
    wo_send,
    wo_recv,
    ws_send,
    ws_recv,
    o_send,
    o_recv,
):
    half = nz // 2
    whole_events = (half - 1) * 4
    events = whole_events + 2
    depth = tok.shape[-1]
    group = NX * rows
    queries = NY * group
    tiles = queries // 128
    out_rows = wo_hbm.shape[0]
    out_cols = wo.shape[-1]

    sp = lax.axis_index("sp")
    y = lax.axis_index("tp")
    c = lax.rem(sp, NC)
    x = lax.rem(sp // NC, NX)
    z = sp // (NC * NX)

    def device(zz, xx, cc, yy):
        return {"sp": (zz * NX + xx) * NC + cc, "tp": yy}

    def around(value, step, count):
        return lax.rem(value + (step % count), count)

    def remote(src, dst, send, recv, where):
        return pltpu.make_async_remote_copy(
            src_ref=src,
            dst_ref=dst,
            send_sem=send,
            recv_sem=recv,
            device_id=where,
            device_id_type=MESH,
        )

    up = device(z, x, c, around(y, 1, NY))
    down = device(z, x, c, around(y, -1, NY))
    right = device(around(z, 1, nz), x, c, y)
    left = device(around(z, -1, nz), x, c, y)
    sibling = device(z, x, 1 - c, y)

    loads = []
    for part in range(2):
        loads.append(
            pltpu.make_async_copy(
                tok_hbm.at[:, pl.ds(part * depth, depth)], tok.at[0, part], load_sem.at[part]
            )
        )
    weight_loads = [
        pltpu.make_async_copy(w, wkvq.at[i], load_sem.at[2 + i])
        for i, w in enumerate((wk_hbm, wv_hbm, wq_hbm))
    ]
    wo_loads = [
        pltpu.make_async_copy(
            wo_hbm.at[:, pl.ds(part * out_cols, out_cols)], wo.at[y, part], load_sem.at[5 + part]
        )
        for part in range(2)
    ]
    for copy in loads + weight_loads + wo_loads:
        copy.start()

    barrier = pltpu.get_barrier_semaphore()
    peers = [right, left, sibling]
    for oy in range(NY):
        for ox in range(NX):
            if (oy, ox) != (0, 0):
                peers.append(device(z, around(x, ox, NX), c, around(y, oy, NY)))
    for peer in peers:
        pl.semaphore_signal(barrier, inc=1, device_id=peer, device_id_type=MESH)
    for copy in loads:
        copy.wait()
    pl.semaphore_wait(barrier, len(peers))

    def y_copy(slot, part):
        return remote(
            tok.at[0, part],
            tok.at[slot, part],
            y_send.at[slot, part],
            y_recv.at[slot, part],
            down if slot == 1 else up,
        )

    def y_relay(part):
        return remote(
            tok.at[2 if part == 0 else 1, part],
            tok.at[3, part],
            y_send.at[3, part],
            y_recv.at[3, part],
            up if part == 0 else down,
        )

    y_copy(2, 0).start()
    y_copy(1, 1).start()
    y_copy(2, 1).start()
    y_copy(1, 0).start()

    def x_copy(s, o, which):
        other = around(x, o, NX)
        source = around(x, -o, NX)
        to = device(z, other, c, y)
        mine = pl.ds(pl.multiple_of(s * group + x * rows, 16), rows)
        theirs = pl.ds(pl.multiple_of(s * group + source * rows, 16), rows)
        span = mine if which < 2 else theirs
        if which % 2 == 0:
            return remote(send_kv.at[s, other], kv.at[0, span], x_send.at[s, o], x_recv.at[s, o], to)
        return remote(send_q.at[s, other], qbuf.at[span], q_send.at[s, o], q_recv.at[s, o], to)

    def project(s):
        first = tok[s, 0]
        second = tok[s, 1]

        def product(i):
            out = jnp.dot(first, wkvq[i, :depth, :], preferred_element_type=F32)
            out += jnp.dot(second, wkvq[i, depth:, :], preferred_element_type=F32)
            return out.astype(BF16)

        mine = pl.ds(pl.multiple_of(s * group + x * rows, 16), rows)
        keys = product(0)
        values = product(1)
        for head in range(NX):
            cols = slice(head * 128, head * 128 + 128)
            send_kv[s, head, :, :128] = keys[:, cols]
            send_kv[s, head, :, 128:] = values[:, cols]
        for o in (2, 1, 3):
            x_copy(s, o, 0).start()
        kv[0, mine, :] = send_kv[s, x]
        found = product(2)
        for head in range(NX):
            send_q[s, head] = found[:, head * 128 : head * 128 + 128]
        for o in (2, 1, 3):
            x_copy(s, o, 1).start()
        qbuf[mine, :] = send_q[s, x]

    def ring_first(s, way):
        if half > 1:
            event = s
        elif (way == 0) == (s < 2):
            event = s % 2
        else:
            return None
        return remote(
            kv.at[0, pl.ds(s * group, group)],
            kv.at[2 + event, pl.ds(way * group, group)],
            r_send.at[s, way],
            r_recv.at[event, way],
            right if way == 0 else left,
        )

    def sibling_first(s):
        span = pl.ds(s * group, group)
        return remote(kv.at[0, span], kv.at[1, span], s_send.at[events + s], s_recv.at[events + s], sibling)

    def launch(s):
        for o in (1, 3, 2):
            x_copy(s, o, 2).wait_recv()
        for way in range(2):
            copy = ring_first(s, way)
            if copy is not None:
                copy.start()
        sibling_first(s).start()

    for copy in weight_loads:
        copy.wait()
    project(0)
    launch(0)
    y_copy(2, 0).wait_recv()
    y_relay(0).start()
    y_copy(1, 1).wait_recv()
    y_relay(1).start()
    y_copy(1, 0).wait_recv()
    project(1)
    y_copy(2, 1).wait_recv()
    project(2)
    launch(1)
    launch(2)

    def wo_span(part):
        size = out_rows // 2
        return pl.ds(part * size, size)

    def wo_copy(way, part):
        span = wo_span(part)
        return remote(
            wo.at[y, c, span],
            wo.at[y, c, span],
            wo_send.at[way, part],
            wo_recv.at[way, part],
            up if way == 0 else down,
        )

    def wo_arrival(way, part):
        origin = around(y, -1 if way == 0 else 1, NY)
        span = wo_span(part)
        return remote(
            wo.at[y, c, span],
            wo.at[origin, c, span],
            wo_send.at[way, part],
            wo_recv.at[way, part],
            up if way == 0 else down,
        )

    def wo_relay(part):
        origin = around(y, -1 if part == 0 else 1, NY)
        span = wo_span(part)
        return remote(
            wo.at[origin, c, span],
            wo.at[origin, c, span],
            wo_send.at[2, part],
            wo_recv.at[2, part],
            up if part == 0 else down,
        )

    def wo_relay_arrival(part):
        origin = around(y, 2, NY)
        span = wo_span(part)
        return remote(
            wo.at[y, c, span],
            wo.at[origin, c, span],
            wo_send.at[2, part],
            wo_recv.at[2, part],
            up if part == 0 else down,
        )

    def wo_sibling(way, part, core):
        origin = around(y, (-1, 1, 2)[way], NY)
        span = wo_span(part)
        return remote(
            wo.at[origin, core, span],
            wo.at[origin, core, span],
            ws_send.at[way, part],
            ws_recv.at[way, part],
            sibling,
        )

    for copy in wo_loads:
        copy.wait()

    y_relay_in = [
        remote(tok.at[0, part], tok.at[3, part], y_send.at[3, part], y_recv.at[3, part], up)
        for part in range(2)
    ]
    for copy in y_relay_in:
        copy.wait_recv()
    wo_copy(0, 0).start()
    wo_copy(1, 1).start()
    wo_copy(0, 1).start()
    wo_copy(1, 0).start()
    project(3)
    launch(3)

    for s in range(NY):
        for o in (1, 3, 2):
            x_copy(s, o, 3).wait_recv()
    upper = lax.broadcasted_iota(jnp.int32, (128, 128), 0) < 64

    def build(t, carry):
        block = qbuf[pl.ds(pl.multiple_of(t * 128, 128), 128), :].astype(F32)
        block = block.T * (64**-0.5 * LOG2E)
        nothing = jnp.zeros_like(block)
        for map_, part in enumerate((jnp.where(upper, block, nothing), jnp.where(upper, nothing, block))):
            high = part.astype(BF16)
            low = (part - high.astype(F32)).astype(BF16)
            qw[t, :128, map_ * 128 : map_ * 128 + 128] = high
            qw[t, 128:, map_ * 128 : map_ * 128 + 128] = low
        return carry

    lax.fori_loop(0, tiles, build, 0)
    top[...] = jnp.full_like(top, -1e30)
    acc[...] = jnp.zeros_like(acc)

    ones = jnp.where(
        lax.broadcasted_iota(jnp.int32, (16, 4 * group), 0) == 0, 1.0, 0.0
    ).astype(BF16)

    def arrival(e, way):
        return remote(
            kv.at[0, pl.ds(0, group)],
            kv.at[2 + e, pl.ds(way * group, group)],
            r_send.at[e, way],
            r_recv.at[e, way],
            right,
        )

    def forward(e, way, target):
        return remote(
            kv.at[2 + e, pl.ds(way * group, group)],
            kv.at[2 + target, pl.ds(way * group, group)],
            r_send.at[4 + e, way],
            r_recv.at[target, way],
            right if way == 0 else left,
        )

    def to_sibling(e):
        return remote(
            kv.at[2 + e, pl.ds(0, 2 * group)],
            kv.at[2 + e, pl.ds(2 * group, 2 * group)],
            s_send.at[e],
            s_recv.at[e],
            sibling,
        )

    def goes_left(e):
        target = jnp.where(e + 4 < whole_events, e + 4, e + 2)
        return (e + 4 < whole_events) | ((e < whole_events) & (lax.rem(e, 4) >= 2)), target

    def receive(e):
        arrival(e, 0).wait_recv()

        @pl.when(e + 4 < events)
        def _():
            forward(e, 0, e + 4).start()

        arrival(e, 1).wait_recv()
        moves, target = goes_left(e)

        @pl.when(moves)
        def _():
            forward(e, 1, target).start()

        to_sibling(e).start()

    def attend(u, carry):
        @pl.when(u == 1)
        def _():
            for s in range(NY):
                sibling_first(s).wait_recv()

        @pl.when(u >= 2)
        def _():
            to_sibling(u - 2).wait_recv()

        keys = kv[u, :, :128]
        keys = jnp.concatenate([keys, keys], axis=1)
        values = jnp.concatenate([kv[u, :, 128:].T, ones], axis=0)
        scores = [jnp.dot(keys, qw[t], preferred_element_type=F32) for t in range(2)]
        waiting = []

        def add():
            t, factor, weights = waiting.pop(0)
            acc[t] = acc[t] * factor + jnp.dot(values, weights, preferred_element_type=F32)

        for t in range(tiles):
            if t + 2 < tiles:
                scores.append(jnp.dot(keys, qw[t + 2], preferred_element_type=F32))
            block = scores.pop(0)
            before = top[t]
            now = jnp.maximum(before, jnp.max(block, axis=0, keepdims=True))
            top[t] = now
            waiting.append((t, jnp.exp2(before - now), jnp.exp2(block - now).astype(BF16)))
            if t > 0:
                add()
        add()
        return carry

    relay_at = events // 2

    def step(e, carry):
        receive(e)

        @pl.when(e == relay_at)
        def _():
            for part in range(2):
                wo_arrival(part, part).wait_recv()
                wo_relay(part).start()
                wo_sibling(part, part, c).start()

        begin = e + jnp.where(e >= 5, 1, 0)
        end = e + 1 + jnp.where(e >= 4, 1, 0)
        lax.fori_loop(begin, end, attend, 0)
        return carry

    lax.fori_loop(0, events, step, 0)
    for way in range(2):
        wo_arrival(way, 1 - way).wait_recv()
        wo_sibling(way, 1 - way, c).start()
    behind = events + (1 if events > 4 else 0)
    lax.fori_loop(behind, events + 2, attend, 0)

    mix = lam_ref[x]
    gain = gain_ref[...]

    def finish(t, carry):
        ratio = acc[t, :128] / acc[t, 128:129]
        heads_out = ratio[:, :128] - mix * ratio[:, 128:]
        meansq = jnp.mean(heads_out * heads_out, axis=0, keepdims=True)
        normed = (heads_out * lax.rsqrt(meansq + 1e-06)).T * gain
        nbuf[pl.ds(pl.multiple_of(t * 128, 128), 128), :] = normed.astype(BF16)
        return carry

    lax.fori_loop(0, tiles, finish, 0, unroll=True)

    def o_copy(s, o, arriving):
        other = around(x, o, NX)
        span = pl.ds(pl.multiple_of(s * group + other * rows, 16), rows)
        if arriving:
            slot = around(y, -Y_OFFSET[s], NY) * NX + around(x, -o, NX)
        else:
            slot = y * NX + x
        return remote(
            nbuf.at[span],
            mixin.at[slot],
            o_send.at[s, o],
            o_recv.at[s, o],
            device(z, other, c, around(y, Y_OFFSET[s], NY)),
        )

    exchanges = [(s, o) for s in (3, 1, 2, 0) for o in (2, 1, 3, 0) if (s, o) != (0, 0)]
    for s, o in exchanges:
        o_copy(s, o, False).start()
    mixin[y * NX + x] = nbuf[pl.ds(pl.multiple_of(x * rows, 16), rows), :]

    for part in range(2):
        wo_relay_arrival(part).wait_recv()
        wo_sibling(2, part, c).start()
    for way in range(3):
        for part in range(2):
            wo_sibling(way, part, 1 - c).wait_recv()
    for s, o in exchanges:
        o_copy(s, o, True).wait_recv()
    normed = jnp.concatenate([mixin[h] for h in range(NX * NY)], axis=1)
    for part in range(2):
        mixed = jnp.zeros((rows, out_cols), F32)
        for yy in range(NY):
            span = slice(yy * out_rows, (yy + 1) * out_rows)
            mixed += jnp.dot(normed[:, span], wo[yy, part], preferred_element_type=F32)
        out_ref[:, part * out_cols : (part + 1) * out_cols] = mixed.astype(BF16)

    for part in range(2):
        for slot in (1, 2):
            y_copy(slot, part).wait_send()
        y_relay(part).wait_send()
    for s in range(NY):
        for o in (1, 2, 3):
            x_copy(s, o, 0).wait_send()
            x_copy(s, o, 1).wait_send()
        for way in range(2):
            copy = ring_first(s, way)
            if copy is not None:
                copy.wait_send()
        sibling_first(s).wait_send()

    def drain(e, carry):
        @pl.when(e + 4 < events)
        def _():
            forward(e, 0, e + 4).wait_send()

        moves, target = goes_left(e)

        @pl.when(moves)
        def _():
            forward(e, 1, target).wait_send()

        to_sibling(e).wait_send()
        return carry

    lax.fori_loop(0, events, drain, 0)
    for part in range(2):
        for way in range(2):
            wo_copy(way, part).wait_send()
        wo_relay(part).wait_send()
        for way in range(3):
            wo_sibling(way, part, c).wait_send()
    for s, o in exchanges:
        o_copy(s, o, False).wait_send()


def solution(mesh):
    nz = mesh.shape["sp"] // (NX * NC)

    def shards(tokens, w_query, w_key, w_value, w_out, mix_weight, out_gain):
        rows, width = tokens.shape
        cols = w_query.shape[1]
        group = NX * rows
        queries = NY * group
        tiles = queries // 128
        events = (nz // 2 - 1) * 4 + 2
        dma = pltpu.SemaphoreType.DMA
        anywhere = pl.BlockSpec(memory_space=pl.ANY)
        return pl.pallas_call(
            functools.partial(kernel, nz, rows),
            out_shape=jax.ShapeDtypeStruct((rows, width), BF16),
            in_specs=[anywhere] * 5
            + [pl.BlockSpec(memory_space=pltpu.SMEM), pl.BlockSpec(memory_space=pltpu.VMEM)],
            out_specs=pl.BlockSpec(memory_space=pltpu.VMEM),
            scratch_shapes=[
                pltpu.VMEM((NY, 2, rows, width // 2), BF16),
                pltpu.VMEM((3, width, cols), BF16),
                pltpu.VMEM((NY, 2, w_out.shape[0], width // 2), BF16),
                pltpu.VMEM((NY, NX, rows, 256), BF16),
                pltpu.VMEM((NY, NX, rows, 128), BF16),
                pltpu.VMEM((queries, 128), BF16),
                pltpu.VMEM((events + 2, 4 * group, 256), BF16),
                pltpu.VMEM((tiles, 256, 256), BF16),
                pltpu.VMEM((tiles, 1, 256), F32),
                pltpu.VMEM((tiles, 144, 256), F32),
                pltpu.VMEM((queries, 128), BF16),
                pltpu.VMEM((NX * NY, rows, 128), BF16),
                dma((7,)),
                dma((4, 2)),
                dma((4, 2)),
                dma((4, 4)),
                dma((4, 4)),
                dma((4, 4)),
                dma((4, 4)),
                dma((events + 4, 2)),
                dma((events, 2)),
                dma((events + 4,)),
                dma((events + 4,)),
                dma((3, 2)),
                dma((3, 2)),
                dma((3, 2)),
                dma((3, 2)),
                dma((4, 4)),
                dma((4, 4)),
            ],
            compiler_params=pltpu.CompilerParams(
                collective_id=0,
                has_side_effects=True,
                vmem_limit_bytes=56 * 1024 * 1024,
            ),
        )(tokens, w_query, w_key, w_value, w_out, mix_weight, out_gain.reshape(1, -1))

    in_specs = (
        P(("sp", "tp"), None),
        P(None, "tp"),
        P(None, "tp"),
        P(None, "tp"),
        P("tp", None),
        P("tp"),
        P(),
    )
    return jax.shard_map(
        shards, mesh=mesh, in_specs=in_specs, out_specs=P(("sp", "tp"), None), check_vma=False
    )
```

```python
import functools

import jax
import jax.numpy as jnp
from jax import lax
from jax.experimental import pallas as pl
from jax.experimental.pallas import tpu as pltpu
from jax.sharding import PartitionSpec as P

MESH = pl.DeviceIdType.MESH
NX = 4
NY = 4
NC = 2
Y_OFFSET = (0, 1, 3, 2)
BF16 = jnp.bfloat16
F32 = jnp.float32
LOG2E = 1.4426950408889634
RIGHT = ((0, 1), (0, 2), (1, 1), (2, 1), (0, 3), (3, 1), (1, 2), (2, 2), (3, 2), (1, 3), (2, 3), (3, 3), (0, 4), (1, 4))
LEFT = RIGHT[:12] + ((2, 4), (3, 4))
EVENTS = len(RIGHT)


def kernel(
    nz,
    rows,
    sem_shapes,
    tok_hbm,
    wq_hbm,
    wk_hbm,
    wv_hbm,
    wo_hbm,
    lam_ref,
    gain_ref,
    out_ref,
    tok,
    wkvq,
    wo,
    send_kv,
    send_q,
    qbuf,
    kv,
    qw,
    top,
    acc,
    nbuf,
    mixin,
):
    def body(
        load_sem,
        y_send,
        y_recv,
        x_send,
        x_recv,
        q_send,
        q_recv,
        r_send,
        r_recv,
        s_send,
        s_recv,
        wo_send,
        wo_recv,
        wx_send,
        wx_recv,
        ws_send,
        ws_recv,
        o_send,
        o_recv,
    ):
        events = EVENTS
        depth = tok.shape[-1]
        group = NX * rows
        queries = NY * group
        tiles = queries // 128
        out_rows = wo_hbm.shape[0]
        out_cols = wo.shape[-1]

        sp = lax.axis_index("sp")
        y = lax.axis_index("tp")
        c = lax.rem(sp, NC)
        x = lax.rem(sp // NC, NX)
        z = sp // (NC * NX)

        def device(zz, xx, cc, yy):
            return {"sp": (zz * NX + xx) * NC + cc, "tp": yy}

        def around(value, step, count):
            return lax.rem(value + (step % count), count)

        def remote(src, dst, send, recv, where):
            return pltpu.make_async_remote_copy(
                src_ref=src,
                dst_ref=dst,
                send_sem=send,
                recv_sem=recv,
                device_id=where,
                device_id_type=MESH,
            )

        up = device(z, x, c, around(y, 1, NY))
        down = device(z, x, c, around(y, -1, NY))
        right = device(around(z, 1, nz), x, c, y)
        left = device(around(z, -1, nz), x, c, y)
        sibling = device(z, x, 1 - c, y)

        loads = []
        for part in range(2):
            loads.append(
                pltpu.make_async_copy(
                    tok_hbm.at[:, pl.ds(part * depth, depth)], tok.at[0, part], load_sem.at[part]
                )
            )
        weight_loads = [
            pltpu.make_async_copy(w, wkvq.at[i], load_sem.at[2 + i])
            for i, w in enumerate((wk_hbm, wv_hbm, wq_hbm))
        ]
        wo_loads = [
            pltpu.make_async_copy(
                wo_hbm.at[:, pl.ds(part * out_cols, out_cols)], wo.at[y, part], load_sem.at[5 + part]
            )
            for part in range(2)
        ]
        for copy in loads:
            copy.start()

        barrier = pltpu.get_barrier_semaphore()
        peers = [up, down, right, left, sibling, device(z, x, c, around(y, 2, NY))]
        peers += [device(z, around(x, ox, NX), c, y) for ox in range(1, NX)]
        for peer in peers:
            pl.semaphore_signal(barrier, inc=1, device_id=peer, device_id_type=MESH)
        for copy in weight_loads + wo_loads:
            copy.start()
        for copy in loads:
            copy.wait()
        pl.semaphore_wait(barrier, len(peers))

        def y_copy(slot):
            step = -Y_OFFSET[slot]
            where = device(z, x, c, around(y, step, NY))
            return remote(tok.at[0], tok.at[slot], y_send.at[slot], y_recv.at[slot], where)

        y_copy(1).start()
        y_copy(2).start()

        def x_copy(s, o, which):
            other = around(x, o, NX)
            source = around(x, -o, NX)
            to = device(z, other, c, y)
            mine = pl.ds(pl.multiple_of(s * group + x * rows, 16), rows)
            theirs = pl.ds(pl.multiple_of(s * group + source * rows, 16), rows)
            span = mine if which < 2 else theirs
            if which % 2 == 0:
                return remote(send_kv.at[s, other], kv.at[0, span], x_send.at[s, o], x_recv.at[s, o], to)
            return remote(send_q.at[s, other], qbuf.at[span], q_send.at[s, o], q_recv.at[s, o], to)

        def project(subs):
            def tokens(part):
                blocks = [tok[s, part] for s in subs]
                return blocks[0] if len(blocks) == 1 else jnp.concatenate(blocks, axis=0)

            first = tokens(0)
            second = tokens(1)

            def product(i):
                out = jnp.dot(first, wkvq[i, :depth, :], preferred_element_type=F32)
                out += jnp.dot(second, wkvq[i, depth:, :], preferred_element_type=F32)
                return out.astype(BF16)

            def mine(s):
                return pl.ds(pl.multiple_of(s * group + x * rows, 16), rows)

            keys = product(0)
            values = product(1)
            for at, s in enumerate(subs):
                span = slice(at * rows, at * rows + rows)
                for head in range(NX):
                    cols = slice(head * 128, head * 128 + 128)
                    send_kv[s, head, :, :128] = keys[span, cols]
                    send_kv[s, head, :, 128:] = values[span, cols]
                for o in (2, 1, 3):
                    x_copy(s, o, 0).start()
                kv[0, mine(s), :] = send_kv[s, x]
            found = product(2)
            for at, s in enumerate(subs):
                for head in range(NX):
                    send_q[s, head] = found[at * rows : at * rows + rows, head * 128 : head * 128 + 128]
                for o in (2, 1, 3):
                    x_copy(s, o, 1).start()
                qbuf[mine(s), :] = send_q[s, x]

        def place(e, way):
            return kv.at[2 + e // 2, pl.ds((e % 2 * 2 + way) * group, group)]

        def ring_first(s, way):
            event = (RIGHT, LEFT)[way].index((s, 1))
            return remote(
                kv.at[0, pl.ds(s * group, group)],
                place(event, way),
                r_send.at[events + s, way],
                r_recv.at[event, way],
                right if way == 0 else left,
            )

        def sibling_first(s):
            span = pl.ds(s * group, group)
            return remote(kv.at[0, span], kv.at[1, span], s_send.at[events + s], s_recv.at[events + s], sibling)

        def launch(s):
            for o in (1, 3, 2):
                x_copy(s, o, 2).wait_recv()
            for way in range(2):
                ring_first(s, way).start()
            sibling_first(s).start()

        size = out_rows // 4
        parity = lax.rem(x, 2)
        east = device(z, around(x, 1, NX), c, y)
        west = device(z, around(x, -1, NX), c, y)
        planes = [around(y, step, NY) for step in (-1, 1, 2)]

        def wo_rows(half_, chunk):
            return pl.ds(pl.multiple_of((half_ * 2 + chunk) * size, 16), size)

        def wo_copy(way, chunk):
            span = wo.at[y, c, wo_rows(parity, chunk)]
            return remote(
                span, span, wo_send.at[way, chunk], wo_recv.at[way, chunk], up if way == 0 else down
            )

        def wo_relay(chunk):
            span = wo.at[planes[chunk], c, wo_rows(parity, chunk)]
            return remote(
                span, span, wo_send.at[2, chunk], wo_recv.at[2, chunk], up if chunk == 0 else down
            )

        def wo_arrival(way, chunk):
            span = wo.at[planes[way], c, wo_rows(parity, chunk)]
            return remote(span, span, wo_send.at[way, chunk], wo_recv.at[way, chunk], up)

        def wo_across(way, chunk):
            span = wo.at[planes[way], c, wo_rows(parity, chunk)]
            return remote(
                span, span, wx_send.at[way, chunk], wx_recv.at[way, chunk], east if chunk == 0 else west
            )

        def wo_across_arrival(way, chunk):
            span = wo.at[planes[way], c, wo_rows(1 - parity, chunk)]
            return remote(span, span, wx_send.at[way, chunk], wx_recv.at[way, chunk], east)

        def wo_sibling(way, core):
            span = wo.at[planes[way], core]
            return remote(span, span, ws_send.at[way], ws_recv.at[way], sibling)

        def wo_pass(way, chunk):
            wo_arrival(way, chunk).wait_recv()
            wo_across(way, chunk).start()

        def arrival(e, way):
            return remote(
                kv.at[0, pl.ds(0, group)], place(e, way), r_send.at[e, way], r_recv.at[e, way], right
            )

        def forward(e, way):
            order = (RIGHT, LEFT)[way]
            piece, distance = order[e]
            if (piece, distance + 1) not in order:
                return None
            target = order.index((piece, distance + 1))
            return remote(
                place(e, way),
                place(target, way),
                r_send.at[e, way],
                r_recv.at[target, way],
                right if way == 0 else left,
            )

        def to_sibling(e):
            span = pl.ds(e % 2 * 2 * group, 2 * group)
            return remote(
                kv.at[2 + e // 2, span], kv.at[9 + e // 2, span], s_send.at[e], s_recv.at[e], sibling
            )

        def receive(e):
            for way in range(2):
                arrival(e, way).wait_recv()
                copy = forward(e, way)
                if copy is not None:
                    copy.start()
            to_sibling(e).start()

        upper = lax.broadcasted_iota(jnp.int32, (128, 128), 0) < 64

        def build(t, carry):
            block = qbuf[pl.ds(pl.multiple_of(t * 128, 128), 128), :].astype(F32)
            block = block.T * (64**-0.5 * LOG2E)
            nothing = jnp.zeros_like(block)
            for map_, part in enumerate((jnp.where(upper, block, nothing), jnp.where(upper, nothing, block))):
                high = part.astype(BF16)
                low = (part - high.astype(F32)).astype(BF16)
                qw[t, :128, map_ * 128 : map_ * 128 + 128] = high
                qw[t, 128:, map_ * 128 : map_ * 128 + 128] = low
            return carry

        def queries_of(subs):
            for s in subs:
                for o in (1, 3, 2):
                    x_copy(s, o, 3).wait_recv()

        for copy in weight_loads:
            copy.wait()
        project([0])
        launch(0)
        y_copy(3).start()
        y_copy(1).wait_recv()
        y_copy(2).wait_recv()
        project([1, 2])
        for copy in wo_loads:
            copy.wait()
        for way, chunk in ((0, 0), (1, 1), (0, 1), (1, 0)):
            wo_copy(way, chunk).start()
        receive(0)
        launch(1)
        launch(2)
        y_copy(3).wait_recv()
        project([3])
        receive(1)
        queries_of((0, 1, 2))
        early = 3 * group // 128
        lax.fori_loop(0, early, build, 0)
        ones = jnp.where(
            lax.broadcasted_iota(jnp.int32, (16, 4 * group), 0) == 0, 1.0, 0.0
        ).astype(BF16)
        top[...] = jnp.full_like(top, -1e30)
        acc[...] = jnp.zeros_like(acc)
        launch(3)
        queries_of((3,))
        lax.fori_loop(early, tiles, build, 0)

        def attend(units):
            for u in units:

                @pl.when(u == 1)
                def _():
                    for s in range(NY):
                        sibling_first(s).wait_recv()

                @pl.when(u >= 9)
                def _():
                    for at in range(2):
                        e = 2 * (u - 9) + at
                        span = pl.ds(at * 2 * group, 2 * group)
                        remote(
                            kv.at[0, span], kv.at[u, span], s_send.at[e], s_recv.at[e], sibling
                        ).wait_recv()

            keys = []
            values = []
            for u in units:
                block = kv[u, :, :128]
                keys.append(jnp.concatenate([block, block], axis=1))
                values.append(jnp.concatenate([kv[u, :, 128:].T, ones], axis=0))
            items = [(i, t) for i in range(len(units)) for t in range(tiles)]

            def score(item):
                i, t = item
                return jnp.dot(keys[i], qw[t], preferred_element_type=F32)

            scores = [score(item) for item in items[:2]]
            waiting = []

            def add():
                i, t, factor, weights = waiting.pop(0)
                acc[t] = acc[t] * factor + jnp.dot(values[i], weights, preferred_element_type=F32)

            for at, (i, t) in enumerate(items):
                if at + 2 < len(items):
                    scores.append(score(items[at + 2]))
                block = scores.pop(0)
                before = top[t]
                now = jnp.maximum(before, jnp.max(block, axis=0, keepdims=True))
                top[t] = now
                waiting.append((i, t, jnp.exp2(before - now), jnp.exp2(block - now).astype(BF16)))
                if at > 0:
                    add()
            add()

        def pick(at, numbers):
            found = jnp.int32(numbers[-1])
            for i in range(len(numbers) - 2, -1, -1):
                found = jnp.where(at == i, numbers[i], found)
            return found

        def step(k, carry):
            @pl.when(k == 1)
            def _():
                receive(2)
                receive(3)
                for way in range(2):
                    wo_arrival(way, way).wait_recv()
                    wo_relay(way).start()
                    wo_across(way, way).start()

            @pl.when(k == 2)
            def _():
                receive(4)
                receive(5)

            @pl.when(k == 3)
            def _():
                receive(6)
                for way in range(2):
                    wo_pass(way, 1 - way)

            attend([pick(k, (0, 3, 1, 10)), pick(k, (2, 9, 4, 11))])
            return carry

        lax.fori_loop(0, 4, step, 0)

        def last(i, carry):
            for at in range(5):

                @pl.when(i == at)
                def _(at=at):
                    receive(7 + at)

            @pl.when(i == 0)
            def _():
                for chunk in range(2):
                    wo_pass(2, chunk)

            @pl.when(i == 6)
            def _():
                receive(12)
                receive(13)

            @pl.when(i == 4)
            def _():
                for way in range(3):
                    for chunk in range(2):
                        wo_across_arrival(way, chunk).wait_recv()
                    wo_sibling(way, c).start()

            attend([pick(i, (5, 12, 6, 13, 7, 14, 8, 15))])
            return carry

        lax.fori_loop(0, 8, last, 0)

        mix = lam_ref[x]
        gain = gain_ref[...]

        def finish(t, carry):
            ratio = acc[t, :128] / acc[t, 128:129]
            heads_out = ratio[:, :128] - mix * ratio[:, 128:]
            meansq = jnp.mean(heads_out * heads_out, axis=0, keepdims=True)
            normed = (heads_out * lax.rsqrt(meansq + 1e-06)).T * gain
            nbuf[pl.ds(pl.multiple_of(t * 128, 128), 128), :] = normed.astype(BF16)
            return carry

        lax.fori_loop(0, tiles, finish, 0, unroll=True)

        def o_copy(s, o, arriving):
            other = around(x, o, NX)
            span = pl.ds(pl.multiple_of(s * group + other * rows, 16), rows)
            if arriving:
                slot = around(y, -Y_OFFSET[s], NY) * NX + around(x, -o, NX)
            else:
                slot = y * NX + x
            return remote(
                nbuf.at[span],
                mixin.at[slot],
                o_send.at[s, o],
                o_recv.at[s, o],
                device(z, other, c, around(y, Y_OFFSET[s], NY)),
            )

        exchanges = [(s, o) for s in (3, 1, 2, 0) for o in (2, 1, 3, 0) if (s, o) != (0, 0)]
        for s, o in exchanges:
            o_copy(s, o, False).start()
        mixin[y * NX + x] = nbuf[pl.ds(pl.multiple_of(x * rows, 16), rows), :]

        for way in range(3):
            wo_sibling(way, 1 - c).wait_recv()
        mixed = [jnp.zeros((rows, out_cols), F32) for _ in range(2)]
        for s in (0, 1, 2, 3):
            for o in (0, 1, 3, 2):
                if (s, o) != (0, 0):
                    o_copy(s, o, True).wait_recv()
            origin = around(y, -Y_OFFSET[s], NY)
            normed = jnp.concatenate([mixin[origin * NX + i] for i in range(NX)], axis=1)
            for part in range(2):
                mixed[part] += jnp.dot(normed, wo[origin, part], preferred_element_type=F32)
        for part in range(2):
            out_ref[:, part * out_cols : (part + 1) * out_cols] = mixed[part].astype(BF16)

        for slot in (1, 2, 3):
            y_copy(slot).wait_send()
        for s in range(NY):
            for o in (1, 2, 3):
                x_copy(s, o, 0).wait_send()
                x_copy(s, o, 1).wait_send()
            for way in range(2):
                ring_first(s, way).wait_send()
            sibling_first(s).wait_send()

        for e in range(events):
            for way in range(2):
                copy = forward(e, way)
                if copy is not None:
                    copy.wait_send()
            to_sibling(e).wait_send()
        for way in range(3):
            for chunk in range(2):
                if way < 2:
                    wo_copy(way, chunk).wait_send()
                wo_across(way, chunk).wait_send()
            wo_sibling(way, c).wait_send()
        for chunk in range(2):
            wo_relay(chunk).wait_send()
        for s, o in exchanges:
            o_copy(s, o, False).wait_send()

    pl.run_scoped(body, *sem_shapes)


def solution(mesh):
    nz = mesh.shape["sp"] // (NX * NC)
    assert nz == 8

    def shards(tokens, w_query, w_key, w_value, w_out, mix_weight, out_gain):
        rows, width = tokens.shape
        cols = w_query.shape[1]
        group = NX * rows
        queries = NY * group
        tiles = queries // 128
        events = EVENTS
        dma = pltpu.SemaphoreType.DMA
        anywhere = pl.BlockSpec(memory_space=pl.ANY)
        semaphores = [
            dma((7,)),
            dma((4,)),
            dma((4,)),
            dma((4, 4)),
            dma((4, 4)),
            dma((4, 4)),
            dma((4, 4)),
            dma((events + 4, 2)),
            dma((events, 2)),
            dma((events + 4,)),
            dma((events + 4,)),
            dma((3, 2)),
            dma((3, 2)),
            dma((3, 2)),
            dma((3, 2)),
            dma((3,)),
            dma((3,)),
            dma((4, 4)),
            dma((4, 4)),
        ]
        return pl.pallas_call(
            functools.partial(kernel, nz, rows, semaphores),
            out_shape=jax.ShapeDtypeStruct((rows, width), BF16),
            in_specs=[anywhere] * 5
            + [pl.BlockSpec(memory_space=pltpu.SMEM), pl.BlockSpec(memory_space=pltpu.VMEM)],
            out_specs=pl.BlockSpec(memory_space=pltpu.VMEM),
            scratch_shapes=[
                pltpu.VMEM((NY, 2, rows, width // 2), BF16),
                pltpu.VMEM((3, width, cols), BF16),
                pltpu.VMEM((NY, 2, w_out.shape[0], width // 2), BF16),
                pltpu.VMEM((NY, NX, rows, 256), BF16),
                pltpu.VMEM((NY, NX, rows, 128), BF16),
                pltpu.VMEM((queries, 128), BF16),
                pltpu.VMEM((events + 2, 4 * group, 256), BF16),
                pltpu.VMEM((tiles, 256, 256), BF16),
                pltpu.VMEM((tiles, 1, 256), F32),
                pltpu.VMEM((tiles, 144, 256), F32),
                pltpu.VMEM((queries, 128), BF16),
                pltpu.VMEM((NX * NY, rows, 128), BF16),
            ],
            compiler_params=pltpu.CompilerParams(
                collective_id=0,
                has_side_effects=True,
                vmem_limit_bytes=56 * 1024 * 1024,
            ),
        )(tokens, w_query, w_key, w_value, w_out, mix_weight, out_gain.reshape(1, -1))

    in_specs = (
        P(("sp", "tp"), None),
        P(None, "tp"),
        P(None, "tp"),
        P(None, "tp"),
        P("tp", None),
        P("tp"),
        P(),
    )
    return jax.shard_map(
        shards, mesh=mesh, in_specs=in_specs, out_specs=P(("sp", "tp"), None), check_vma=False
    )
```

```python
import functools

import jax
import jax.numpy as jnp
from jax import lax
from jax.experimental import pallas as pl
from jax.experimental.pallas import tpu as pltpu
from jax.sharding import PartitionSpec as P

MESH = pl.DeviceIdType.MESH
NX = 4
NY = 4
NC = 2
Y_OFFSET = (0, 1, 3, 2)
BF16 = jnp.bfloat16
F32 = jnp.float32
LOG2E = 1.4426950408889634
RIGHT = ((0, 1), (0, 2), (1, 1), (2, 1), (0, 3), (3, 1), (1, 2), (2, 2), (3, 2), (1, 3), (2, 3), (3, 3), (0, 4), (1, 4))
LEFT = RIGHT[:12] + ((2, 4), (3, 4))
EVENTS = len(RIGHT)


def kernel(
    nz,
    rows,
    sem_shapes,
    tok_hbm,
    wq_hbm,
    wk_hbm,
    wv_hbm,
    wo_hbm,
    lam_ref,
    gain_ref,
    out_ref,
    tok,
    wkvq,
    wo,
    send_kv,
    send_q,
    qbuf,
    kv,
    qw,
    top,
    acc,
    nbuf,
    mixin,
):
    def body(
        load_sem,
        y_send,
        y_recv,
        x_send,
        x_recv,
        q_send,
        q_recv,
        r_send,
        r_recv,
        s_send,
        s_recv,
        wo_send,
        wo_recv,
        wx_send,
        wx_recv,
        ws_send,
        ws_recv,
        o_send,
        o_recv,
    ):
        events = EVENTS
        depth = tok.shape[-1]
        group = NX * rows
        queries = NY * group
        tiles = queries // 128
        out_rows = wo_hbm.shape[0]
        out_cols = wo.shape[-1]

        sp = lax.axis_index("sp")
        y = lax.axis_index("tp")
        c = lax.rem(sp, NC)
        x = lax.rem(sp // NC, NX)
        z = sp // (NC * NX)

        def device(zz, xx, cc, yy):
            return {"sp": (zz * NX + xx) * NC + cc, "tp": yy}

        def around(value, step, count):
            return lax.rem(value + (step % count), count)

        def remote(src, dst, send, recv, where):
            return pltpu.make_async_remote_copy(
                src_ref=src,
                dst_ref=dst,
                send_sem=send,
                recv_sem=recv,
                device_id=where,
                device_id_type=MESH,
            )

        up = device(z, x, c, around(y, 1, NY))
        down = device(z, x, c, around(y, -1, NY))
        right = device(around(z, 1, nz), x, c, y)
        left = device(around(z, -1, nz), x, c, y)
        sibling = device(z, x, 1 - c, y)

        loads = []
        for part in range(2):
            loads.append(
                pltpu.make_async_copy(
                    tok_hbm.at[:, pl.ds(part * depth, depth)], tok.at[0, part], load_sem.at[part]
                )
            )
        weight_loads = [
            pltpu.make_async_copy(w, wkvq.at[i], load_sem.at[2 + i])
            for i, w in enumerate((wk_hbm, wv_hbm, wq_hbm))
        ]
        wo_loads = [
            pltpu.make_async_copy(
                wo_hbm.at[:, pl.ds(part * out_cols, out_cols)], wo.at[y, part], load_sem.at[5 + part]
            )
            for part in range(2)
        ]
        for copy in loads:
            copy.start()

        barrier = pltpu.get_barrier_semaphore()
        peers = [up, down, right, left, sibling, device(z, x, c, around(y, 2, NY))]
        peers += [device(z, around(x, ox, NX), c, y) for ox in range(1, NX)]
        for peer in peers:
            pl.semaphore_signal(barrier, inc=1, device_id=peer, device_id_type=MESH)
        for copy in weight_loads + wo_loads:
            copy.start()
        for copy in loads:
            copy.wait()
        pl.semaphore_wait(barrier, len(peers))

        def y_copy(slot):
            step = -Y_OFFSET[slot]
            where = device(z, x, c, around(y, step, NY))
            return remote(tok.at[0], tok.at[slot], y_send.at[slot], y_recv.at[slot], where)

        y_copy(1).start()
        y_copy(2).start()

        def x_copy(s, o, which):
            other = around(x, o, NX)
            source = around(x, -o, NX)
            to = device(z, other, c, y)
            mine = pl.ds(pl.multiple_of(s * group + x * rows, 16), rows)
            theirs = pl.ds(pl.multiple_of(s * group + source * rows, 16), rows)
            span = mine if which < 2 else theirs
            if which % 2 == 0:
                return remote(send_kv.at[s, other], kv.at[0, span], x_send.at[s, o], x_recv.at[s, o], to)
            return remote(send_q.at[s, other], qbuf.at[span], q_send.at[s, o], q_recv.at[s, o], to)

        def project(subs):
            def tokens(part):
                blocks = [tok[s, part] for s in subs]
                return blocks[0] if len(blocks) == 1 else jnp.concatenate(blocks, axis=0)

            first = tokens(0)
            second = tokens(1)

            def product(i):
                out = jnp.dot(first, wkvq[i, :depth, :], preferred_element_type=F32)
                out += jnp.dot(second, wkvq[i, depth:, :], preferred_element_type=F32)
                return out.astype(BF16)

            def mine(s):
                return pl.ds(pl.multiple_of(s * group + x * rows, 16), rows)

            keys = product(0)
            values = product(1)
            for at, s in enumerate(subs):
                span = slice(at * rows, at * rows + rows)
                for head in range(NX):
                    cols = slice(head * 128, head * 128 + 128)
                    send_kv[s, head, :, :128] = keys[span, cols]
                    send_kv[s, head, :, 128:] = values[span, cols]
                for o in (2, 1, 3):
                    x_copy(s, o, 0).start()
                kv[0, mine(s), :] = send_kv[s, x]
            found = product(2)
            for at, s in enumerate(subs):
                for head in range(NX):
                    send_q[s, head] = found[at * rows : at * rows + rows, head * 128 : head * 128 + 128]
                for o in (2, 1, 3):
                    x_copy(s, o, 1).start()
                qbuf[mine(s), :] = send_q[s, x]

        def place(e, way):
            return kv.at[2 + e // 2, pl.ds((e % 2 * 2 + way) * group, group)]

        def ring_first(s, way):
            event = (RIGHT, LEFT)[way].index((s, 1))
            return remote(
                kv.at[0, pl.ds(s * group, group)],
                place(event, way),
                r_send.at[events + s, way],
                r_recv.at[event, way],
                right if way == 0 else left,
            )

        def sibling_first(s):
            span = pl.ds(s * group, group)
            return remote(kv.at[0, span], kv.at[1, span], s_send.at[events + s], s_recv.at[events + s], sibling)

        def launch(s):
            for o in (1, 3, 2):
                x_copy(s, o, 2).wait_recv()
            for way in range(2):
                ring_first(s, way).start()
            sibling_first(s).start()

        size = out_rows // 4
        parity = lax.rem(x, 2)
        east = device(z, around(x, 1, NX), c, y)
        west = device(z, around(x, -1, NX), c, y)
        planes = [around(y, step, NY) for step in (-1, 1, 2)]

        def wo_rows(half_, chunk):
            return pl.ds(pl.multiple_of((half_ * 2 + chunk) * size, 16), size)

        def wo_copy(way, chunk):
            span = wo.at[y, c, wo_rows(parity, chunk)]
            return remote(
                span, span, wo_send.at[way, chunk], wo_recv.at[way, chunk], up if way == 0 else down
            )

        def wo_relay(chunk):
            span = wo.at[planes[chunk], c, wo_rows(parity, chunk)]
            return remote(
                span, span, wo_send.at[2, chunk], wo_recv.at[2, chunk], up if chunk == 0 else down
            )

        def wo_arrival(way, chunk):
            span = wo.at[planes[way], c, wo_rows(parity, chunk)]
            return remote(span, span, wo_send.at[way, chunk], wo_recv.at[way, chunk], up)

        def wo_across(way, chunk):
            span = wo.at[planes[way], c, wo_rows(parity, chunk)]
            return remote(
                span, span, wx_send.at[way, chunk], wx_recv.at[way, chunk], east if chunk == 0 else west
            )

        def wo_across_arrival(way, chunk):
            span = wo.at[planes[way], c, wo_rows(1 - parity, chunk)]
            return remote(span, span, wx_send.at[way, chunk], wx_recv.at[way, chunk], east)

        def wo_sibling(way, core):
            span = wo.at[planes[way], core]
            return remote(span, span, ws_send.at[way], ws_recv.at[way], sibling)

        def wo_pass(way, chunk):
            wo_arrival(way, chunk).wait_recv()
            wo_across(way, chunk).start()

        def arrival(e, way):
            return remote(
                kv.at[0, pl.ds(0, group)], place(e, way), r_send.at[e, way], r_recv.at[e, way], right
            )

        def forward(e, way):
            order = (RIGHT, LEFT)[way]
            piece, distance = order[e]
            if (piece, distance + 1) not in order:
                return None
            target = order.index((piece, distance + 1))
            return remote(
                place(e, way),
                place(target, way),
                r_send.at[e, way],
                r_recv.at[target, way],
                right if way == 0 else left,
            )

        def to_sibling(e):
            span = pl.ds(e % 2 * 2 * group, 2 * group)
            return remote(
                kv.at[2 + e // 2, span], kv.at[9 + e // 2, span], s_send.at[e], s_recv.at[e], sibling
            )

        def receive(e):
            for way in range(2):
                arrival(e, way).wait_recv()
                copy = forward(e, way)
                if copy is not None:
                    copy.start()
            to_sibling(e).start()

        upper = lax.broadcasted_iota(jnp.int32, (128, 128), 0) < 64

        def build(t, carry):
            block = qbuf[pl.ds(pl.multiple_of(t * 128, 128), 128), :].astype(F32)
            block = block.T * (64**-0.5 * LOG2E)
            nothing = jnp.zeros_like(block)
            for map_, part in enumerate((jnp.where(upper, block, nothing), jnp.where(upper, nothing, block))):
                high = part.astype(BF16)
                low = (part - high.astype(F32)).astype(BF16)
                qw[t, :128, map_ * 128 : map_ * 128 + 128] = high
                qw[t, 128:, map_ * 128 : map_ * 128 + 128] = low
            return carry

        def queries_of(subs):
            for s in subs:
                for o in (1, 3, 2):
                    x_copy(s, o, 3).wait_recv()

        for copy in weight_loads:
            copy.wait()
        project([0])
        launch(0)
        y_copy(3).start()
        y_copy(1).wait_recv()
        y_copy(2).wait_recv()
        project([1, 2])
        for copy in wo_loads:
            copy.wait()
        for way, chunk in ((0, 0), (1, 1), (0, 1), (1, 0)):
            wo_copy(way, chunk).start()
        receive(0)
        launch(1)
        launch(2)
        y_copy(3).wait_recv()
        project([3])
        receive(1)
        queries_of((0, 1, 2))
        early = 3 * group // 128
        lax.fori_loop(0, early, build, 0)
        ones = jnp.where(
            lax.broadcasted_iota(jnp.int32, (16, 4 * group), 0) == 0, 1.0, 0.0
        ).astype(BF16)
        top[...] = jnp.full_like(top, -1e30)
        acc[...] = jnp.zeros_like(acc)
        launch(3)
        queries_of((3,))
        lax.fori_loop(early, tiles, build, 0)

        def attend(units):
            for u in units:

                @pl.when(u == 1)
                def _():
                    for s in range(NY):
                        sibling_first(s).wait_recv()

                @pl.when(u >= 9)
                def _():
                    for at in range(2):
                        e = 2 * (u - 9) + at
                        span = pl.ds(at * 2 * group, 2 * group)
                        remote(
                            kv.at[0, span], kv.at[u, span], s_send.at[e], s_recv.at[e], sibling
                        ).wait_recv()

            keys = []
            values = []
            for u in units:
                block = kv[u, :, :128]
                keys.append(jnp.concatenate([block, block], axis=1))
                values.append(jnp.concatenate([kv[u, :, 128:].T, ones], axis=0))
            items = [(i, t) for i in range(len(units)) for t in range(tiles)]

            def score(item):
                i, t = item
                return jnp.dot(keys[i], qw[t], preferred_element_type=F32)

            scores = [score(item) for item in items[:2]]
            waiting = []

            def add():
                i, t, factor, weights = waiting.pop(0)
                acc[t] = acc[t] * factor + jnp.dot(values[i], weights, preferred_element_type=F32)

            for at, (i, t) in enumerate(items):
                if at + 2 < len(items):
                    scores.append(score(items[at + 2]))
                block = scores.pop(0)
                before = top[t]
                now = jnp.maximum(before, jnp.max(block, axis=0, keepdims=True))
                top[t] = now
                waiting.append((i, t, jnp.exp2(before - now), jnp.exp2(block - now).astype(BF16)))
                if at > 0:
                    add()
            add()

        def pick(at, numbers):
            found = jnp.int32(numbers[-1])
            for i in range(len(numbers) - 2, -1, -1):
                found = jnp.where(at == i, numbers[i], found)
            return found

        def step(k, carry):
            @pl.when(k == 1)
            def _():
                receive(2)
                receive(3)
                for way in range(2):
                    wo_arrival(way, way).wait_recv()
                    wo_relay(way).start()
                    wo_across(way, way).start()

            @pl.when(k == 2)
            def _():
                receive(4)
                receive(5)

            @pl.when(k == 3)
            def _():
                receive(6)
                receive(7)
                for way in range(2):
                    wo_pass(way, 1 - way)

            attend([pick(k, (0, 3, 1, 10)), pick(k, (2, 9, 4, 5))])
            return carry

        lax.fori_loop(0, 4, step, 0)

        def last(i, carry):
            for at in range(4):

                @pl.when(i == at)
                def _(at=at):
                    receive(8 + at)

            @pl.when(i == 0)
            def _():
                for chunk in range(2):
                    wo_pass(2, chunk)

            @pl.when(i == 6)
            def _():
                receive(12)
                receive(13)

            @pl.when(i == 4)
            def _():
                for way in range(3):
                    for chunk in range(2):
                        wo_across_arrival(way, chunk).wait_recv()
                    wo_sibling(way, c).start()

            attend([pick(i, (11, 6, 12, 7, 13, 14, 8, 15))])
            return carry

        lax.fori_loop(0, 8, last, 0)

        mix = lam_ref[x]
        gain = gain_ref[...]

        def finish(t, carry):
            ratio = acc[t, :128] / acc[t, 128:129]
            heads_out = ratio[:, :128] - mix * ratio[:, 128:]
            meansq = jnp.mean(heads_out * heads_out, axis=0, keepdims=True)
            normed = (heads_out * lax.rsqrt(meansq + 1e-06)).T * gain
            nbuf[pl.ds(pl.multiple_of(t * 128, 128), 128), :] = normed.astype(BF16)
            return carry

        lax.fori_loop(0, tiles, finish, 0, unroll=True)

        def o_copy(s, o, arriving):
            other = around(x, o, NX)
            span = pl.ds(pl.multiple_of(s * group + other * rows, 16), rows)
            if arriving:
                slot = around(y, -Y_OFFSET[s], NY) * NX + around(x, -o, NX)
            else:
                slot = y * NX + x
            return remote(
                nbuf.at[span],
                mixin.at[slot],
                o_send.at[s, o],
                o_recv.at[s, o],
                device(z, other, c, around(y, Y_OFFSET[s], NY)),
            )

        exchanges = [(s, o) for s in (3, 1, 2, 0) for o in (2, 1, 3, 0) if (s, o) != (0, 0)]
        for s, o in exchanges:
            o_copy(s, o, False).start()
        mixin[y * NX + x] = nbuf[pl.ds(pl.multiple_of(x * rows, 16), rows), :]

        for way in range(3):
            wo_sibling(way, 1 - c).wait_recv()
        mixed = [jnp.zeros((rows, out_cols), F32) for _ in range(2)]
        for s in (0, 1, 2, 3):
            for o in (0, 1, 3, 2):
                if (s, o) != (0, 0):
                    o_copy(s, o, True).wait_recv()
            origin = around(y, -Y_OFFSET[s], NY)
            normed = jnp.concatenate([mixin[origin * NX + i] for i in range(NX)], axis=1)
            for part in range(2):
                mixed[part] += jnp.dot(normed, wo[origin, part], preferred_element_type=F32)
        for part in range(2):
            out_ref[:, part * out_cols : (part + 1) * out_cols] = mixed[part].astype(BF16)

        for slot in (1, 2, 3):
            y_copy(slot).wait_send()
        for s in range(NY):
            for o in (1, 2, 3):
                x_copy(s, o, 0).wait_send()
                x_copy(s, o, 1).wait_send()
            for way in range(2):
                ring_first(s, way).wait_send()
            sibling_first(s).wait_send()

        for e in range(events):
            for way in range(2):
                copy = forward(e, way)
                if copy is not None:
                    copy.wait_send()
            to_sibling(e).wait_send()
        for way in range(3):
            for chunk in range(2):
                if way < 2:
                    wo_copy(way, chunk).wait_send()
                wo_across(way, chunk).wait_send()
            wo_sibling(way, c).wait_send()
        for chunk in range(2):
            wo_relay(chunk).wait_send()
        for s, o in exchanges:
            o_copy(s, o, False).wait_send()

    pl.run_scoped(body, *sem_shapes)


def solution(mesh):
    nz = mesh.shape["sp"] // (NX * NC)
    assert nz == 8

    def shards(tokens, w_query, w_key, w_value, w_out, mix_weight, out_gain):
        rows, width = tokens.shape
        cols = w_query.shape[1]
        group = NX * rows
        queries = NY * group
        tiles = queries // 128
        events = EVENTS
        dma = pltpu.SemaphoreType.DMA
        anywhere = pl.BlockSpec(memory_space=pl.ANY)
        semaphores = [
            dma((7,)),
            dma((4,)),
            dma((4,)),
            dma((4, 4)),
            dma((4, 4)),
            dma((4, 4)),
            dma((4, 4)),
            dma((events + 4, 2)),
            dma((events, 2)),
            dma((events + 4,)),
            dma((events + 4,)),
            dma((3, 2)),
            dma((3, 2)),
            dma((3, 2)),
            dma((3, 2)),
            dma((3,)),
            dma((3,)),
            dma((4, 4)),
            dma((4, 4)),
        ]
        return pl.pallas_call(
            functools.partial(kernel, nz, rows, semaphores),
            out_shape=jax.ShapeDtypeStruct((rows, width), BF16),
            in_specs=[anywhere] * 5
            + [pl.BlockSpec(memory_space=pltpu.SMEM), pl.BlockSpec(memory_space=pltpu.VMEM)],
            out_specs=pl.BlockSpec(memory_space=pltpu.VMEM),
            scratch_shapes=[
                pltpu.VMEM((NY, 2, rows, width // 2), BF16),
                pltpu.VMEM((3, width, cols), BF16),
                pltpu.VMEM((NY, 2, w_out.shape[0], width // 2), BF16),
                pltpu.VMEM((NY, NX, rows, 256), BF16),
                pltpu.VMEM((NY, NX, rows, 128), BF16),
                pltpu.VMEM((queries, 128), BF16),
                pltpu.VMEM((events + 2, 4 * group, 256), BF16),
                pltpu.VMEM((tiles, 256, 256), BF16),
                pltpu.VMEM((tiles, 1, 256), F32),
                pltpu.VMEM((tiles, 144, 256), F32),
                pltpu.VMEM((queries, 128), BF16),
                pltpu.VMEM((NX * NY, rows, 128), BF16),
            ],
            compiler_params=pltpu.CompilerParams(
                collective_id=0,
                has_side_effects=True,
                vmem_limit_bytes=56 * 1024 * 1024,
            ),
        )(tokens, w_query, w_key, w_value, w_out, mix_weight, out_gain.reshape(1, -1))

    in_specs = (
        P(("sp", "tp"), None),
        P(None, "tp"),
        P(None, "tp"),
        P(None, "tp"),
        P("tp", None),
        P("tp"),
        P(),
    )
    return jax.shard_map(
        shards, mesh=mesh, in_specs=in_specs, out_specs=P(("sp", "tp"), None), check_vma=False
    )
```

```python
import functools

import jax
import jax.numpy as jnp
from jax import lax
from jax.experimental import pallas as pl
from jax.experimental.pallas import tpu as pltpu
from jax.sharding import PartitionSpec as P

MESH = pl.DeviceIdType.MESH
NX = 4
NY = 4
NC = 2
Y_OFFSET = (0, 1, 3, 2)
BF16 = jnp.bfloat16
F32 = jnp.float32
LOG2E = 1.4426950408889634
RIGHT = ((0, 1), (0, 2), (1, 1), (2, 1), (0, 3), (3, 1), (1, 2), (2, 2), (3, 2), (1, 3), (2, 3), (3, 3), (0, 4), (1, 4))
LEFT = RIGHT[:12] + ((2, 4), (3, 4))
EVENTS = len(RIGHT)


def kernel(
    nz,
    rows,
    sem_shapes,
    tok_hbm,
    wq_hbm,
    wk_hbm,
    wv_hbm,
    wo_hbm,
    lam_ref,
    gain_ref,
    out_ref,
    tok,
    wkvq,
    wo,
    send_kv,
    send_q,
    qbuf,
    kv,
    qw,
    top,
    acc,
    nbuf,
    mixin,
    result,
):
    def body(
        load_sem,
        y_send,
        y_recv,
        x_send,
        x_recv,
        q_send,
        q_recv,
        r_send,
        r_recv,
        s_send,
        s_recv,
        wo_send,
        wo_recv,
        wx_send,
        wx_recv,
        ws_send,
        ws_recv,
        o_send,
        o_recv,
    ):
        events = EVENTS
        depth = tok.shape[-1]
        group = NX * rows
        queries = NY * group
        tiles = queries // 128
        out_rows = wo_hbm.shape[0]
        out_cols = wo.shape[-1]

        sp = lax.axis_index("sp")
        y = lax.axis_index("tp")
        c = lax.rem(sp, NC)
        x = lax.rem(sp // NC, NX)
        z = sp // (NC * NX)

        def device(zz, xx, cc, yy):
            return {"sp": (zz * NX + xx) * NC + cc, "tp": yy}

        def around(value, step, count):
            return lax.rem(value + (step % count), count)

        def remote(src, dst, send, recv, where):
            return pltpu.make_async_remote_copy(
                src_ref=src,
                dst_ref=dst,
                send_sem=send,
                recv_sem=recv,
                device_id=where,
                device_id_type=MESH,
            )

        up = device(z, x, c, around(y, 1, NY))
        down = device(z, x, c, around(y, -1, NY))
        right = device(around(z, 1, nz), x, c, y)
        left = device(around(z, -1, nz), x, c, y)
        sibling = device(z, x, 1 - c, y)

        loads = []
        for part in range(2):
            loads.append(
                pltpu.make_async_copy(
                    tok_hbm.at[:, pl.ds(part * depth, depth)], tok.at[0, part], load_sem.at[part]
                )
            )
        weight_loads = [
            pltpu.make_async_copy(w, wkvq.at[i], load_sem.at[2 + i])
            for i, w in enumerate((wk_hbm, wv_hbm, wq_hbm))
        ]
        wo_loads = [
            pltpu.make_async_copy(
                wo_hbm.at[:, pl.ds(part * out_cols, out_cols)], wo.at[y, part], load_sem.at[5 + part]
            )
            for part in range(2)
        ]
        for copy in loads:
            copy.start()

        barrier = pltpu.get_barrier_semaphore()
        peers = [up, down, right, left, sibling, device(z, x, c, around(y, 2, NY))]
        peers += [device(z, around(x, ox, NX), c, y) for ox in range(1, NX)]
        for peer in peers:
            pl.semaphore_signal(barrier, inc=1, device_id=peer, device_id_type=MESH)
        for copy in weight_loads + wo_loads:
            copy.start()
        for copy in loads:
            copy.wait()
        pl.semaphore_wait(barrier, len(peers))

        def y_copy(slot, part):
            step = -Y_OFFSET[slot]
            where = device(z, x, c, around(y, step, NY))
            return remote(
                tok.at[0, part], tok.at[slot, part], y_send.at[slot, part], y_recv.at[slot, part], where
            )

        for part in range(2):
            y_copy(1, part).start()
            y_copy(2, part).start()

        def x_copy(s, o, which):
            other = around(x, o, NX)
            source = around(x, -o, NX)
            to = device(z, other, c, y)
            mine = pl.ds(pl.multiple_of(s * group + x * rows, 16), rows)
            theirs = pl.ds(pl.multiple_of(s * group + source * rows, 16), rows)
            span = mine if which < 2 else theirs
            if which % 2 == 0:
                return remote(send_kv.at[s, other], kv.at[0, span], x_send.at[s, o], x_recv.at[s, o], to)
            return remote(send_q.at[s, other], qbuf.at[span], q_send.at[s, o], q_recv.at[s, o], to)

        def project(subs):
            def tokens(part):
                blocks = [tok[s, part] for s in subs]
                return blocks[0] if len(blocks) == 1 else jnp.concatenate(blocks, axis=0)

            def arrive(part):
                for s in subs:
                    if s:
                        y_copy(s, part).wait_recv()

            def product(i, part, block):
                weights = wkvq[i, part * depth : (part + 1) * depth, :]
                return jnp.dot(block, weights, preferred_element_type=F32)

            arrive(0)
            first = tokens(0)
            sums = [product(i, 0, first) for i in range(3)]
            arrive(1)
            second = tokens(1)

            def mine(s):
                return pl.ds(pl.multiple_of(s * group + x * rows, 16), rows)

            keys = (sums[0] + product(0, 1, second)).astype(BF16)
            values = (sums[1] + product(1, 1, second)).astype(BF16)
            for at, s in enumerate(subs):
                span = slice(at * rows, at * rows + rows)
                for head in range(NX):
                    cols = slice(head * 128, head * 128 + 128)
                    send_kv[s, head, :, :128] = keys[span, cols]
                    send_kv[s, head, :, 128:] = values[span, cols]
                for o in (2, 1, 3):
                    x_copy(s, o, 0).start()
                kv[0, mine(s), :] = send_kv[s, x]
            found = (sums[2] + product(2, 1, second)).astype(BF16)
            for at, s in enumerate(subs):
                for head in range(NX):
                    send_q[s, head] = found[at * rows : at * rows + rows, head * 128 : head * 128 + 128]
                for o in (2, 1, 3):
                    x_copy(s, o, 1).start()
                qbuf[mine(s), :] = send_q[s, x]

        def place(e, way):
            return kv.at[2 + e // 2, pl.ds((e % 2 * 2 + way) * group, group)]

        def ring_first(s, way):
            event = (RIGHT, LEFT)[way].index((s, 1))
            return remote(
                kv.at[0, pl.ds(s * group, group)],
                place(event, way),
                r_send.at[events + s, way],
                r_recv.at[event, way],
                right if way == 0 else left,
            )

        def sibling_first(s):
            span = pl.ds(s * group, group)
            return remote(kv.at[0, span], kv.at[1, span], s_send.at[events + s], s_recv.at[events + s], sibling)

        def launch(s):
            for o in (1, 3, 2):
                x_copy(s, o, 2).wait_recv()
            for way in range(2):
                ring_first(s, way).start()
            sibling_first(s).start()

        size = out_rows // 4
        parity = lax.rem(x, 2)
        east = device(z, around(x, 1, NX), c, y)
        west = device(z, around(x, -1, NX), c, y)
        planes = [around(y, step, NY) for step in (-1, 1, 2)]

        def wo_rows(half_, chunk):
            return pl.ds(pl.multiple_of((half_ * 2 + chunk) * size, 16), size)

        def wo_copy(way, chunk):
            span = wo.at[y, c, wo_rows(parity, chunk)]
            return remote(
                span, span, wo_send.at[way, chunk], wo_recv.at[way, chunk], up if way == 0 else down
            )

        def wo_relay(chunk):
            span = wo.at[planes[chunk], c, wo_rows(parity, chunk)]
            return remote(
                span, span, wo_send.at[2, chunk], wo_recv.at[2, chunk], up if chunk == 0 else down
            )

        def wo_arrival(way, chunk):
            span = wo.at[planes[way], c, wo_rows(parity, chunk)]
            return remote(span, span, wo_send.at[way, chunk], wo_recv.at[way, chunk], up)

        def wo_across(way, chunk):
            span = wo.at[planes[way], c, wo_rows(parity, chunk)]
            return remote(
                span, span, wx_send.at[way, chunk], wx_recv.at[way, chunk], east if chunk == 0 else west
            )

        def wo_across_arrival(way, chunk):
            span = wo.at[planes[way], c, wo_rows(1 - parity, chunk)]
            return remote(span, span, wx_send.at[way, chunk], wx_recv.at[way, chunk], east)

        def wo_sibling(way, core):
            span = wo.at[planes[way], core]
            return remote(span, span, ws_send.at[way], ws_recv.at[way], sibling)

        def wo_pass(way, chunk):
            wo_arrival(way, chunk).wait_recv()
            wo_across(way, chunk).start()

        def arrival(e, way):
            return remote(
                kv.at[0, pl.ds(0, group)], place(e, way), r_send.at[e, way], r_recv.at[e, way], right
            )

        def forward(e, way):
            order = (RIGHT, LEFT)[way]
            piece, distance = order[e]
            if (piece, distance + 1) not in order:
                return None
            target = order.index((piece, distance + 1))
            return remote(
                place(e, way),
                place(target, way),
                r_send.at[e, way],
                r_recv.at[target, way],
                right if way == 0 else left,
            )

        def to_sibling(e):
            span = pl.ds(e % 2 * 2 * group, 2 * group)
            return remote(
                kv.at[2 + e // 2, span], kv.at[9 + e // 2, span], s_send.at[e], s_recv.at[e], sibling
            )

        def receive(e):
            for way in range(2):
                arrival(e, way).wait_recv()
                copy = forward(e, way)
                if copy is not None:
                    copy.start()
            to_sibling(e).start()

        upper = lax.broadcasted_iota(jnp.int32, (128, 128), 0) < 64

        def build(t, carry):
            block = qbuf[pl.ds(pl.multiple_of(t * 128, 128), 128), :].astype(F32)
            block = block.T * (64**-0.5 * LOG2E)
            nothing = jnp.zeros_like(block)
            for map_, part in enumerate((jnp.where(upper, block, nothing), jnp.where(upper, nothing, block))):
                high = part.astype(BF16)
                low = (part - high.astype(F32)).astype(BF16)
                qw[t, :128, map_ * 128 : map_ * 128 + 128] = high
                qw[t, 128:, map_ * 128 : map_ * 128 + 128] = low
            return carry

        def queries_of(subs):
            for s in subs:
                for o in (1, 3, 2):
                    x_copy(s, o, 3).wait_recv()

        for copy in weight_loads:
            copy.wait()
        project([0])
        launch(0)
        for part in range(2):
            y_copy(3, part).start()
        project([1, 2])
        for copy in wo_loads:
            copy.wait()
        for way, chunk in ((0, 0), (1, 1), (0, 1), (1, 0)):
            wo_copy(way, chunk).start()
        receive(0)
        launch(1)
        launch(2)
        project([3])
        receive(1)
        queries_of((0, 1, 2))
        early = 3 * group // 128
        lax.fori_loop(0, early, build, 0)
        ones = jnp.where(
            lax.broadcasted_iota(jnp.int32, (16, 4 * group), 0) == 0, 1.0, 0.0
        ).astype(BF16)
        top[...] = jnp.full_like(top, -1e30)
        acc[...] = jnp.zeros_like(acc)
        launch(3)
        queries_of((3,))
        lax.fori_loop(early, tiles, build, 0)

        def attend(units):
            for u in units:

                @pl.when(u == 1)
                def _():
                    for s in range(NY):
                        sibling_first(s).wait_recv()

                @pl.when(u >= 9)
                def _():
                    for at in range(2):
                        e = 2 * (u - 9) + at
                        span = pl.ds(at * 2 * group, 2 * group)
                        remote(
                            kv.at[0, span], kv.at[u, span], s_send.at[e], s_recv.at[e], sibling
                        ).wait_recv()

            keys = []
            values = []
            for u in units:
                block = kv[u, :, :128]
                keys.append(jnp.concatenate([block, block], axis=1))
                values.append(jnp.concatenate([kv[u, :, 128:].T, ones], axis=0))
            items = [(i, t) for i in range(len(units)) for t in range(tiles)]

            def score(item):
                i, t = item
                return jnp.dot(keys[i], qw[t], preferred_element_type=F32)

            scores = [score(item) for item in items[:2]]
            waiting = []

            def add():
                i, t, factor, weights = waiting.pop(0)
                acc[t] = acc[t] * factor + jnp.dot(values[i], weights, preferred_element_type=F32)

            for at, (i, t) in enumerate(items):
                if at + 2 < len(items):
                    scores.append(score(items[at + 2]))
                block = scores.pop(0)
                before = top[t]
                now = jnp.maximum(before, jnp.max(block, axis=0, keepdims=True))
                top[t] = now
                waiting.append((i, t, jnp.exp2(before - now), jnp.exp2(block - now).astype(BF16)))
                if at > 0:
                    add()
            add()

        def pick(at, numbers):
            found = jnp.int32(numbers[-1])
            for i in range(len(numbers) - 2, -1, -1):
                found = jnp.where(at == i, numbers[i], found)
            return found

        def step(k, carry):
            @pl.when(k == 1)
            def _():
                receive(2)
                receive(3)
                for way in range(2):
                    wo_arrival(way, way).wait_recv()
                    wo_relay(way).start()
                    wo_across(way, way).start()

            @pl.when(k == 2)
            def _():
                receive(4)
                receive(5)

            @pl.when(k == 3)
            def _():
                receive(6)
                for way in range(2):
                    wo_pass(way, 1 - way)

            attend([pick(k, (0, 3, 1, 10)), pick(k, (2, 9, 4, 11))])
            return carry

        lax.fori_loop(0, 4, step, 0)

        def last(i, carry):
            for at in range(5):

                @pl.when(i == at)
                def _(at=at):
                    receive(7 + at)

            @pl.when(i == 0)
            def _():
                for chunk in range(2):
                    wo_pass(2, chunk)

            @pl.when(i == 6)
            def _():
                receive(12)
                receive(13)

            @pl.when(i == 4)
            def _():
                for way in range(3):
                    for chunk in range(2):
                        wo_across_arrival(way, chunk).wait_recv()
                    wo_sibling(way, c).start()

            attend([pick(i, (5, 12, 6, 13, 7, 14, 8, 15))])
            return carry

        lax.fori_loop(0, 8, last, 0)

        mix = lam_ref[x]
        gain = gain_ref[...]

        def finish(t, carry):
            ratio = acc[t, :128] / acc[t, 128:129]
            heads_out = ratio[:, :128] - mix * ratio[:, 128:]
            meansq = jnp.mean(heads_out * heads_out, axis=0, keepdims=True)
            normed = (heads_out * lax.rsqrt(meansq + 1e-06)).T * gain
            nbuf[pl.ds(pl.multiple_of(t * 128, 128), 128), :] = normed.astype(BF16)
            return carry

        lax.fori_loop(0, tiles, finish, 0, unroll=True)

        def o_copy(s, o, arriving):
            other = around(x, o, NX)
            span = pl.ds(pl.multiple_of(s * group + other * rows, 16), rows)
            if arriving:
                slot = around(y, -Y_OFFSET[s], NY) * NX + around(x, -o, NX)
            else:
                slot = y * NX + x
            return remote(
                nbuf.at[span],
                mixin.at[slot],
                o_send.at[s, o],
                o_recv.at[s, o],
                device(z, other, c, around(y, Y_OFFSET[s], NY)),
            )

        exchanges = [(s, o) for s in (3, 1, 2, 0) for o in (2, 1, 3, 0) if (s, o) != (0, 0)]
        for s, o in exchanges:
            o_copy(s, o, False).start()
        mixin[y * NX + x] = nbuf[pl.ds(pl.multiple_of(x * rows, 16), rows), :]

        for way in range(3):
            wo_sibling(way, 1 - c).wait_recv()
        mixed = [jnp.zeros((rows, out_cols), F32) for _ in range(2)]
        for s in (0, 1, 2, 3):
            for o in (0, 1, 3, 2):
                if (s, o) != (0, 0):
                    o_copy(s, o, True).wait_recv()
            origin = around(y, -Y_OFFSET[s], NY)
            normed = jnp.concatenate([mixin[origin * NX + i] for i in range(NX)], axis=1)
            for part in range(2):
                mixed[part] += jnp.dot(normed, wo[origin, part], preferred_element_type=F32)
        stores = []
        for part in range(2):
            cols = slice(part * out_cols, (part + 1) * out_cols)
            result[:, cols] = mixed[part].astype(BF16)
            span = pl.ds(part * out_cols, out_cols)
            stores.append(
                pltpu.make_async_copy(result.at[:, span], out_ref.at[:, span], load_sem.at[part])
            )
            stores[-1].start()

        for copy in stores:
            copy.wait()
        for slot in (1, 2, 3):
            for part in range(2):
                y_copy(slot, part).wait_send()
        for s in range(NY):
            for o in (1, 2, 3):
                x_copy(s, o, 0).wait_send()
                x_copy(s, o, 1).wait_send()
            for way in range(2):
                ring_first(s, way).wait_send()
            sibling_first(s).wait_send()

        for e in range(events):
            for way in range(2):
                copy = forward(e, way)
                if copy is not None:
                    copy.wait_send()
            to_sibling(e).wait_send()
        for way in range(3):
            for chunk in range(2):
                if way < 2:
                    wo_copy(way, chunk).wait_send()
                wo_across(way, chunk).wait_send()
            wo_sibling(way, c).wait_send()
        for chunk in range(2):
            wo_relay(chunk).wait_send()
        for s, o in exchanges:
            o_copy(s, o, False).wait_send()

    pl.run_scoped(body, *sem_shapes)


def solution(mesh):
    nz = mesh.shape["sp"] // (NX * NC)
    assert nz == 8

    def shards(tokens, w_query, w_key, w_value, w_out, mix_weight, out_gain):
        rows, width = tokens.shape
        cols = w_query.shape[1]
        group = NX * rows
        queries = NY * group
        tiles = queries // 128
        events = EVENTS
        dma = pltpu.SemaphoreType.DMA
        anywhere = pl.BlockSpec(memory_space=pl.ANY)
        semaphores = [
            dma((7,)),
            dma((4, 2)),
            dma((4, 2)),
            dma((4, 4)),
            dma((4, 4)),
            dma((4, 4)),
            dma((4, 4)),
            dma((events + 4, 2)),
            dma((events, 2)),
            dma((events + 4,)),
            dma((events + 4,)),
            dma((3, 2)),
            dma((3, 2)),
            dma((3, 2)),
            dma((3, 2)),
            dma((3,)),
            dma((3,)),
            dma((4, 4)),
            dma((4, 4)),
        ]
        return pl.pallas_call(
            functools.partial(kernel, nz, rows, semaphores),
            out_shape=jax.ShapeDtypeStruct((rows, width), BF16),
            in_specs=[anywhere] * 5
            + [pl.BlockSpec(memory_space=pltpu.SMEM), pl.BlockSpec(memory_space=pltpu.VMEM)],
            out_specs=anywhere,
            scratch_shapes=[
                pltpu.VMEM((NY, 2, rows, width // 2), BF16),
                pltpu.VMEM((3, width, cols), BF16),
                pltpu.VMEM((NY, 2, w_out.shape[0], width // 2), BF16),
                pltpu.VMEM((NY, NX, rows, 256), BF16),
                pltpu.VMEM((NY, NX, rows, 128), BF16),
                pltpu.VMEM((queries, 128), BF16),
                pltpu.VMEM((events + 2, 4 * group, 256), BF16),
                pltpu.VMEM((tiles, 256, 256), BF16),
                pltpu.VMEM((tiles, 1, 256), F32),
                pltpu.VMEM((tiles, 144, 256), F32),
                pltpu.VMEM((queries, 128), BF16),
                pltpu.VMEM((NX * NY, rows, 128), BF16),
                pltpu.VMEM((rows, width), BF16),
            ],
            compiler_params=pltpu.CompilerParams(
                collective_id=0,
                has_side_effects=True,
                vmem_limit_bytes=56 * 1024 * 1024,
            ),
        )(tokens, w_query, w_key, w_value, w_out, mix_weight, out_gain.reshape(1, -1))

    in_specs = (
        P(("sp", "tp"), None),
        P(None, "tp"),
        P(None, "tp"),
        P(None, "tp"),
        P("tp", None),
        P("tp"),
        P(),
    )
    return jax.shard_map(
        shards, mesh=mesh, in_specs=in_specs, out_specs=P(("sp", "tp"), None), check_vma=False
    )
```
